32 devices in a mesh: dp: 2 (over x), kv: 8 (over z, y), tp: 2 (over core).
Axes of the slice: x: 2, y: 2, z: 4, core: 2. Of those that a mesh axis runs over, the one named last changes fastest.
Arguments:
- tokens: bfloat16 [32, 3072], P(('tp', 'dp'), 'kv'), parts along dimension 0, may hold values from -60 to 60
- old_state: float32 [32, 24, 128, 128], P(('tp', 'dp', 'kv')), parts along dimension 0, may hold values from -0.6 to 0.6
- mixer_gain: float32 [3072], replicated, may hold values from 0.1 to 1.9
- w_query: bfloat16 [3072, 3072], P(None, 'kv'), may hold values from -0.109375 to 0.109375
- w_key: bfloat16 [3072, 3072], P(None, 'kv'), may hold values from -0.109375 to 0.109375
- w_value: bfloat16 [3072, 3072], P(None, 'kv'), may hold values from -0.109375 to 0.109375
- w_outgate: bfloat16 [3072, 3072], P(None, 'kv'), may hold values from -0.109375 to 0.109375
- w_decay: bfloat16 [3072, 24], replicated, may hold values from -0.109375 to 0.109375
- w_write: bfloat16 [3072, 24], replicated, may hold values from -0.109375 to 0.109375
- decay_log: float32 [24], replicated, may hold values from -3 to 1
- decay_bias: float32 [24], replicated, may hold values from -3 to 3
- head_gain: float32 [128], replicated, may hold values from 0.1 to 1.9
- w_output: bfloat16 [3072, 3072], P('kv'), may hold values from -0.15625 to 0.15625
- channel_gain: float32 [3072], replicated, may hold values from 0.1 to 1.9
- w_gate: bfloat16 [3072, 8448], P(None, 'kv'), may hold values from -0.109375 to 0.109375
- w_up: bfloat16 [3072, 8448], P(None, 'kv'), may hold values from -0.109375 to 0.109375
- w_down: bfloat16 [8448, 3072], P(None, 'kv'), may hold values from -0.0625 to 0.0625
Outputs:
- mixed: bfloat16 [32, 3072], P(('tp', 'dp'), 'kv'), parts along dimension 0
- new_state: float32 [32, 24, 128, 128], P(('tp', 'dp', 'kv')), parts along dimension 0
The draws below stay inside these ranges and needn't reach their ends.
There are 2 independent parts, one for each index of `tp`. The reference program is written for one: setup_inputs(seed, part) draws one part's arguments, and reference() takes and returns one part's arrays. A program takes and returns all parts, laid end to end along the dimension named above; an argument that names none is the same for every part. Nothing has to cross between parts.
All inputs are finite; a program needn't handle non-finite values.
Results may differ from the reference program's by a relative error of at most 0.0059.
Values may be sent and summed in bfloat16 or wider, within the bound.
No kernel may reach another device: no remote copies, remote signals or barrier semaphores. Data moves between devices by JAX's collectives and lax.ppermute only.
A program may use at most 64 MiB of HBM per device.

```python
import jax
import jax.numpy as jnp
from jax import lax

D = 3072
HEADS = 24
HEAD_DIM = 128
FF = 8448
BATCH = 16


def draw_tokens(key, part):
    row_key, rough_key, normal_key = jax.random.split(key, 3)
    row_scale = jnp.exp(jax.random.uniform(row_key, (BATCH, 1), jnp.float32, jnp.log(0.3), jnp.log(3.0)))
    position_ramp = jnp.arange(D, dtype=jnp.float32) / D
    rough_factor = jax.random.uniform(rough_key, (D,), jnp.float32, 0.6, 1.4)
    column_scale = jnp.exp(jnp.log(0.4) + jnp.log(8.0) * position_ramp) * rough_factor
    normal_part = jax.random.truncated_normal(normal_key, -4.0, 4.0, (BATCH, D), jnp.float32)
    return (normal_part * row_scale * column_scale[None, :]).astype(jnp.bfloat16)


def spiked(entries, key, source, target, parts, factor):
    owner, partner = [(jnp.arange(entries.shape[dim]) // (entries.shape[dim] // parts)).reshape([-1 if axis == dim else 1 for axis in range(entries.ndim)]) for dim in (source, target)]
    chosen = jax.random.permutation(key, parts)[partner]
    strong = (owner == chosen) | (owner == (partner + parts // 2) % parts)
    return jnp.where(strong, factor * entries, entries)


def level_of(key, shape, cuts, least, top_value):
    def one(position, parts):
        heights = jax.random.uniform(jax.random.fold_in(jax.random.fold_in(key, 6), position), (parts,), jnp.float32, least / len(cuts), top_value / len(cuts))
        return jnp.repeat(jnp.exp(heights), shape[position] // parts).reshape((-1,) + (1,) * (len(shape) - position - 1))

    level = one(*cuts[0])
    for cut in cuts[1:]:
        level = level * one(*cut)
    return level


def gaussian(rng, dims, scale, most, pieces=(), kind=jnp.bfloat16):
    values = jax.random.normal(rng, dims, jnp.float32) * scale
    if len(pieces) > 0:
        values = level_of(rng, dims, pieces, -0.22, 0.18) * values
    return jnp.clip(values, min=-most, max=most).astype(kind)


def bell_draw_with(key, extent, scale, limit, pieces, heavy, kind=jnp.bfloat16):
    values = scale * jax.random.normal(key, extent, jnp.float32)
    if pieces:
        values = values * level_of(key, extent, pieces, -0.22, 0.18)
    return jnp.clip(spiked(values, jax.random.fold_in(key, 3), *heavy), -limit, limit).astype(kind)


def setup_inputs(seed: int = 0, part: int = 0) -> dict:
    keys = jax.random.split(jax.random.key(seed), 18)
    own_keys = jax.random.split(jax.random.fold_in(keys[17], part), 18)
    return {
        "tokens": draw_tokens(jax.random.fold_in(jax.random.fold_in(keys[17], part), 71), part),
        "old_state": gaussian(own_keys[1], (BATCH, HEADS, HEAD_DIM, HEAD_DIM), 0.1, 0.6, ((0, 16),), jnp.float32),
        "mixer_gain": jnp.clip(1.0 + 0.18 * jax.random.normal(keys[2], (D,), jnp.float32), 0.1, 1.9),
        "w_query": gaussian(keys[3], (D, HEADS * HEAD_DIM), D ** -0.5, 0.109375, ((1, 8),)),
        "w_key": gaussian(keys[4], (D, HEADS * HEAD_DIM), D ** -0.5, 0.109375, ((1, 8),)),
        "w_value": gaussian(keys[5], (D, HEADS * HEAD_DIM), D ** -0.5, 0.109375, ((1, 8),)),
        "w_outgate": gaussian(keys[6], (D, HEADS * HEAD_DIM), D ** -0.5, 0.109375, ((1, 8),)),
        "w_decay": gaussian(keys[7], (D, HEADS), D ** -0.5, 0.109375),
        "w_write": gaussian(keys[8], (D, HEADS), D ** -0.5, 0.109375),
        "decay_log": jnp.clip(jax.random.uniform(keys[9], (HEADS,), jnp.float32, -3.0, 1.0), -3.0, 1.0),
        "decay_bias": gaussian(keys[10], (HEADS,), 1.0, 3.0, (), jnp.float32),
        "head_gain": jnp.clip(1.0 + 0.18 * jax.random.normal(keys[11], (HEAD_DIM,), jnp.float32), 0.1, 1.9),
        "w_output": bell_draw_with(keys[12], (HEADS * HEAD_DIM, D), (HEADS * HEAD_DIM) ** -0.5, 0.15625, ((0, 8),), (0, 1, 8, 2.0)),
        "channel_gain": jnp.clip(1.0 + 0.18 * jax.random.normal(keys[13], (D,), jnp.float32), 0.1, 1.9),
        "w_gate": gaussian(keys[14], (D, FF), D ** -0.5, 0.109375, ((1, 8),)),
        "w_up": gaussian(keys[15], (D, FF), D ** -0.5, 0.109375, ((1, 8),)),
        "w_down": gaussian(keys[16], (FF, D), FF ** -0.5, 0.0625, ((1, 8),)),
    }


EPS = 1e-06

def norm_scale(values):
    return lax.rsqrt(lax.optimization_barrier(jnp.mean(values * values, axis=-1, keepdims=True)) + EPS)

def unit_rows(values):
    return values * lax.rsqrt(lax.optimization_barrier(jnp.sum(values * values, axis=-1, keepdims=True)) + EPS)

def sequence_update(packed_blocks):
    previous_state, query_vector, key_vector, value_vec, retain, strength = packed_blocks
    recalled_values = jnp.einsum('gfy,gf->gy', previous_state, key_vector, precision=lax.Precision.HIGHEST)
    correction = value_vec - retain[:, None] * recalled_values
    updated_state = retain[:, None, None] * previous_state + (strength[:, None] * key_vector)[:, :, None] * correction[:, None, :]
    state_readout = jnp.einsum('gfy,gf->gy', updated_state, query_vector, precision=lax.Precision.HIGHEST)
    return (updated_state, state_readout)

def reference(tokens, old_state, mixer_gain, w_query, w_key, w_value, w_outgate, w_decay, w_write, decay_log, decay_bias, head_gain, w_output, channel_gain, w_gate, w_up, w_down):
    batch_rows = tokens.shape[0]
    tok_wide = tokens.astype(jnp.float32)
    scale_in = norm_scale(tok_wide)
    normed = (tok_wide * mixer_gain).astype(jnp.bfloat16)

    def project(weight):
        return jnp.dot(normed, weight, preferred_element_type=jnp.float32) * scale_in

    def by_head(values):
        return values.astype(jnp.float32).reshape(batch_rows, HEADS, HEAD_DIM)
    query_pre = project(w_query).astype(jnp.bfloat16)
    key_pre = project(w_key).astype(jnp.bfloat16)
    value_pre = project(w_value).astype(jnp.bfloat16)
    outgate_pre = project(w_outgate).astype(jnp.bfloat16)
    decay_pre = project(w_decay)
    write_pre = project(w_write)
    queries = unit_rows(jax.nn.silu(by_head(query_pre))) * HEAD_DIM ** (-0.5)
    keys_unit = unit_rows(jax.nn.silu(by_head(key_pre)))
    values_act = jax.nn.silu(by_head(value_pre))
    strength = jax.nn.sigmoid(write_pre)
    retain = jnp.exp(-jnp.exp(decay_log) * jax.nn.softplus(decay_pre + decay_bias))
    new_state, state_readout = lax.map(sequence_update, (old_state, queries, keys_unit, values_act, retain, strength))
    gated_read = state_readout * norm_scale(state_readout) * head_gain * jax.nn.silu(by_head(outgate_pre))
    gated_read = gated_read.reshape(batch_rows, HEADS * HEAD_DIM).astype(jnp.bfloat16)
    mixer_out = jnp.dot(gated_read, w_output, preferred_element_type=jnp.float32)
    residual = lax.optimization_barrier((tok_wide + mixer_out).astype(jnp.bfloat16))
    residual_wide = residual.astype(jnp.float32)
    scale_mid = norm_scale(residual_wide)
    normed_mid = (residual_wide * channel_gain).astype(jnp.bfloat16)
    gate_act = jnp.dot(normed_mid, w_gate, preferred_element_type=jnp.float32) * scale_mid
    upward = jnp.dot(normed_mid, w_up, preferred_element_type=jnp.float32) * scale_mid
    hidden_units = (jax.nn.silu(gate_act) * upward).astype(jnp.bfloat16)
    down_sum = jnp.dot(hidden_units, w_down, preferred_element_type=jnp.float32)
    mixed = (residual_wide + down_sum).astype(jnp.bfloat16)
    return (mixed, new_state)
```

```python
import jax
import jax.numpy as jnp
from jax import lax
from jax.sharding import PartitionSpec as P

HEAD_DIM = 128
EPS = 1e-06


def norm_scale(values):
    return lax.rsqrt(jnp.mean(values * values, axis=-1, keepdims=True) + EPS)


def unit_rows(values):
    return values * lax.rsqrt(jnp.sum(values * values, axis=-1, keepdims=True) + EPS)


def gather_kv(block, parts):
    copies = jnp.broadcast_to(block[None], (parts,) + block.shape)
    return lax.all_to_all(copies, "kv", split_axis=0, concat_axis=0, tiled=True)


def body(
    tokens,
    old_state,
    mixer_gain,
    w_query,
    w_key,
    w_value,
    w_outgate,
    w_decay,
    w_write,
    decay_log,
    decay_bias,
    head_gain,
    w_output,
    channel_gain,
    w_gate,
    w_up,
    w_down,
    *,
    parts,
):
    f32, bf16 = jnp.float32, jnp.bfloat16
    rows, share = tokens.shape
    width = share * parts
    local_rows, heads = old_state.shape[:2]
    head_cols = w_query.shape[1]
    place = lax.axis_index("kv")

    tok_wide = gather_kv(tokens, parts).transpose(1, 0, 2).reshape(rows, width).astype(f32)
    scale_in = norm_scale(tok_wide)
    normed = (tok_wide * mixer_gain).astype(bf16)

    def project(weight):
        return (jnp.dot(normed, weight, preferred_element_type=f32) * scale_in).astype(bf16)

    packed = jnp.stack([project(w) for w in (w_query, w_key, w_value, w_outgate)], axis=1)
    packed = packed.reshape(parts, local_rows, 4, head_cols)
    packed = lax.all_to_all(packed, "kv", split_axis=0, concat_axis=0, tiled=True)

    own_normed = lax.dynamic_slice_in_dim(normed, place * local_rows, local_rows, 0)
    own_scale = lax.dynamic_slice_in_dim(scale_in, place * local_rows, local_rows, 0)
    decay_pre = jnp.dot(own_normed, w_decay, preferred_element_type=f32) * own_scale
    write_pre = jnp.dot(own_normed, w_write, preferred_element_type=f32) * own_scale

    def by_head(index):
        chosen = packed[:, :, index].transpose(1, 0, 2)
        return chosen.reshape(local_rows, heads, HEAD_DIM).astype(f32)

    queries = unit_rows(jax.nn.silu(by_head(0))) * HEAD_DIM ** (-0.5)
    keys_unit = unit_rows(jax.nn.silu(by_head(1)))
    values_act = jax.nn.silu(by_head(2))
    strength = jax.nn.sigmoid(write_pre)
    retain = jnp.exp(-jnp.exp(decay_log) * jax.nn.softplus(decay_pre + decay_bias))
    recalled = jnp.einsum("bhkv,bhk->bhv", old_state, keys_unit, precision=lax.Precision.HIGHEST)
    correction = values_act - retain[..., None] * recalled
    new_state = (
        retain[..., None, None] * old_state
        + (strength[..., None] * keys_unit)[..., :, None] * correction[..., None, :]
    )
    readout = jnp.einsum("bhkv,bhk->bhv", new_state, queries, precision=lax.Precision.HIGHEST)
    gated_read = readout * norm_scale(readout) * head_gain * jax.nn.silu(by_head(3))
    gated_read = gated_read.reshape(local_rows, parts, head_cols).astype(bf16).transpose(1, 0, 2)
    read_cols = lax.all_to_all(gated_read, "kv", split_axis=0, concat_axis=0, tiled=True)
    read_cols = read_cols.reshape(rows, head_cols)

    partial_out = jnp.dot(read_cols, w_output, preferred_element_type=f32)
    partial_out = partial_out.reshape(rows, parts, share).transpose(1, 0, 2)
    mixer_out = lax.all_to_all(partial_out, "kv", split_axis=0, concat_axis=0, tiled=True).sum(0)
    own_residual = (tokens.astype(f32) + mixer_out).astype(bf16)
    residual = gather_kv(own_residual, parts).transpose(1, 0, 2).reshape(rows, width)
    residual_wide = residual.astype(f32)
    scale_mid = norm_scale(residual_wide)
    normed_mid = (residual_wide * channel_gain).astype(bf16)
    gate_act = jnp.dot(normed_mid, w_gate, preferred_element_type=f32) * scale_mid
    upward = jnp.dot(normed_mid, w_up, preferred_element_type=f32) * scale_mid
    hidden = (jax.nn.silu(gate_act) * upward).astype(bf16)
    hidden = gather_kv(hidden, parts).transpose(1, 0, 2).reshape(rows, -1)
    down_sum = jnp.dot(hidden, w_down, preferred_element_type=f32)
    mixed = (own_residual.astype(f32) + down_sum).astype(bf16)
    return (mixed, new_state)


def solution(mesh):
    parts = mesh.shape["kv"]
    rows, states = P(("tp", "dp"), "kv"), P(("tp", "dp", "kv"), None, None, None)
    cols = P(None, "kv")
    in_specs = (rows, states, P(), cols, cols, cols, cols, P(), P(), P(), P(), P())
    in_specs += (P("kv", None), P(), cols, cols, cols)

    def step(*args):
        return body(*args, parts=parts)

    return jax.shard_map(
        step, mesh=mesh, in_specs=in_specs, out_specs=(rows, states), check_vma=False
    )
```

```python
import functools

import jax
import jax.numpy as jnp
from jax import lax
from jax.experimental import pallas as pl
from jax.experimental.pallas import tpu as pltpu
from jax.sharding import PartitionSpec as P

HEAD_DIM = 128
EPS = 1e-06
MIB = 1 << 20
SLOTS = 16

F32, BF16 = jnp.float32, jnp.bfloat16


def norm_scale(values):
    return lax.rsqrt(jnp.mean(values * values, axis=-1, keepdims=True) + EPS)


def unit_rows(values):
    return values * lax.rsqrt(jnp.sum(values * values, axis=-1, keepdims=True) + EPS)


def silu(values):
    return values / (1.0 + jnp.exp(-values))


def exchange(slabs):
    return lax.all_to_all(slabs, "kv", split_axis=0, concat_axis=0, tiled=True)


def gather_kv(block, parts):
    return exchange(jnp.broadcast_to(block[None], (parts,) + block.shape))


def call(kernel, out_shape, args, *, limit=8, scratch=(), spaces=None, span=8):
    vmem = pl.BlockSpec(memory_space=pltpu.VMEM)
    specs = [vmem] * len(args) if spaces is None else spaces
    many = isinstance(out_shape, (tuple, list))
    return pl.pallas_call(
        kernel,
        out_shape=out_shape,
        in_specs=specs,
        out_specs=[vmem] * len(out_shape) if many else vmem,
        scratch_shapes=list(scratch),
        compiler_params=pltpu.CompilerParams(vmem_limit_bytes=limit * MIB),
        cost_estimate=pl.CostEstimate(
            flops=span * 500_000_000, bytes_accessed=span * 3_000_000, transcendentals=0
        ),
    )(*args)


def wide_rows(ref, parts):
    return jnp.concatenate([ref[s] for s in range(parts)], axis=-1)


def eye(n):
    across = lax.broadcasted_iota(jnp.int32, (n, n), 1)
    return lax.broadcasted_iota(jnp.int32, (n, n), 0) == across


def upright(row):
    return jnp.sum(jnp.where(eye(row.shape[1]), row, 0.0), axis=1, keepdims=True)


def spread_kernel(block_ref, out_ref, *, parts):
    for s in range(parts):
        out_ref[s] = block_ref[...]


def project_kernel(
    x_ref, gain_ref, wq, wk, wv, wg, wd_ref, ww_ref, log_ref, bias_ref,
    slab_ref, retain_ref, strength_ref, scr, *, parts, tiles,
):
    x = wide_rows(x_ref, parts).astype(F32)
    scale = norm_scale(x)
    normed = (x * gain_ref[...]).astype(BF16)
    scr[:, 4 * tiles :, :] = jnp.zeros((x.shape[0], SLOTS - 4 * tiles, HEAD_DIM), F32)
    for i, w in enumerate((wq, wk, wv, wg)):
        acc = jnp.dot(normed, w[...], preferred_element_type=F32) * scale
        for t in range(tiles):
            scr[:, i * tiles + t, :] = acc[:, t * HEAD_DIM : (t + 1) * HEAD_DIM]
    slab_ref[...] = scr[...].astype(BF16)
    lane_scale = jnp.sum(jnp.where(eye(x.shape[0]), scale, 0.0), axis=0, keepdims=True)
    nt = (((1,), (1,)), ((), ()))
    decay = lax.dot_general(wd_ref[...], normed, nt, preferred_element_type=F32) * lane_scale
    write = lax.dot_general(ww_ref[...], normed, nt, preferred_element_type=F32) * lane_scale
    pre = decay + upright(bias_ref[...])
    soft = jnp.maximum(pre, 0.0) + jnp.log1p(jnp.exp(-jnp.abs(pre)))
    retain_ref[...] = jnp.exp(-jnp.exp(upright(log_ref[...])) * soft)
    strength_ref[...] = 1.0 / (1.0 + jnp.exp(-write))


def state_kernel(
    place_ref, slab_ref, s_ref, retain_ref, strength_ref, gain_ref,
    read_ref, new_ref, ro, *, parts, tiles,
):
    place = place_ref[0]
    act = silu(slab_ref[...].astype(F32))
    total = jnp.sum(act * act, axis=-1, keepdims=True)
    slot = lax.broadcasted_iota(jnp.int32, act.shape[:2] + (1,), 1)
    factor = lax.rsqrt(total + EPS)
    factor = jnp.where(slot < tiles, factor * HEAD_DIM ** (-0.5), factor)
    factor = jnp.where(slot < 2 * tiles, factor, 1.0)
    unit = act * factor
    ro[...] = jnp.zeros(ro.shape, F32)
    columns = unit.reshape(parts * SLOTS, HEAD_DIM).T
    lane = lax.broadcasted_iota(jnp.int32, retain_ref.shape, 1)
    own = lane == place
    retain = jnp.sum(jnp.where(own, retain_ref[...], 0.0), axis=1, keepdims=True)
    strength = jnp.sum(jnp.where(own, strength_ref[...], 0.0), axis=1, keepdims=True)
    heads = parts * tiles
    retain = jnp.broadcast_to(retain, (heads, HEAD_DIM))
    strength = jnp.broadcast_to(strength, (heads, HEAD_DIM))
    for h in range(heads):
        j, t = divmod(h, tiles)
        base = j * SLOTS + t
        query = columns[:, base : base + 1]
        key = columns[:, base + tiles : base + tiles + 1]
        value = unit[j, 2 * tiles + t : 2 * tiles + t + 1, :]
        old = s_ref[h]
        keep = retain[h : h + 1, :]
        recalled = jnp.sum(old * key, axis=0, keepdims=True)
        correction = (value - keep * recalled) * strength[h : h + 1, :]
        new = keep * old + key * correction
        new_ref[h] = new
        ro[j, 3 * tiles + t : 3 * tiles + t + 1, :] = jnp.sum(new * query, axis=0, keepdims=True)
    readout = ro[...]
    gated = readout * norm_scale(readout) * gain_ref[...] * unit
    read_ref[...] = gated[:, SLOTS // 2 :, :].astype(BF16).astype(F32)


def output_kernel(read_ref, w_ref, out_ref, *, parts, tiles):
    first = 3 * tiles - SLOTS // 2
    rows = jnp.concatenate([read_ref[:, first + t, :] for t in range(tiles)], axis=-1)
    part = jnp.dot(rows.astype(BF16), w_ref[...], preferred_element_type=F32).astype(BF16)
    for s in range(parts):
        out_ref[s] = part


def mixer_kernel(part_ref, x_ref, gain_ref, wg_ref, wu_ref, hid_ref, res_ref, *, parts):
    total = part_ref[0].astype(F32)
    for s in range(1, parts):
        total = total + part_ref[s].astype(F32)
    residual = (wide_rows(x_ref, parts).astype(F32) + total).astype(BF16)
    share = x_ref.shape[2]
    for s in range(parts):
        res_ref[s] = residual[:, s * share : (s + 1) * share]
    wide = residual.astype(F32)
    scale = norm_scale(wide)
    normed = (wide * gain_ref[...]).astype(BF16)
    nt = (((1,), (1,)), ((), ()))
    gate = lax.dot_general(normed, wg_ref[...], nt, preferred_element_type=F32) * scale
    up = lax.dot_general(normed, wu_ref[...], nt, preferred_element_type=F32) * scale
    hidden = (silu(gate) * up).astype(BF16)
    for s in range(parts):
        hid_ref[s] = hidden


def down_kernel(place_ref, hid_ref, res_ref, w_ref, out_ref, *, parts):
    units = hid_ref.shape[2]
    total = res_ref[place_ref[0]].astype(F32)
    for s in range(parts):
        total = total + jnp.dot(
            hid_ref[s], w_ref[s * units : (s + 1) * units, :], preferred_element_type=F32
        )
    out_ref[...] = total.astype(BF16)


def fast_body(
    tokens, old_state, mixer_gain, w_query, w_key, w_value, w_outgate, w_decay, w_write,
    decay_log, decay_bias, head_gain, w_output, channel_gain, w_gate, w_up, w_down, *, parts,
):
    rows, share = tokens.shape
    width = share * parts
    heads = old_state.shape[1]
    tiles = share // HEAD_DIM
    units = w_gate.shape[1]
    shape = jax.ShapeDtypeStruct
    place = lax.axis_index("kv").astype(jnp.int32).reshape(1)
    smem = pl.BlockSpec(memory_space=pltpu.SMEM)
    vmem = pl.BlockSpec(memory_space=pltpu.VMEM)

    tokens, place = lax.optimization_barrier((tokens, place))
    copies = call(
        functools.partial(spread_kernel, parts=parts),
        shape((parts, rows, share), BF16),
        (tokens,),
    )
    x = exchange(copies)
    slab, retain, strength = call(
        functools.partial(project_kernel, parts=parts, tiles=tiles),
        (
            shape((rows, SLOTS, HEAD_DIM), BF16),
            shape((heads, rows), F32),
            shape((heads, rows), F32),
        ),
        (
            x, mixer_gain.reshape(1, width), w_query, w_key, w_value, w_outgate,
            w_decay.T, w_write.T, decay_log.reshape(1, heads), decay_bias.reshape(1, heads),
        ),
        scratch=[pltpu.VMEM((rows, SLOTS, HEAD_DIM), F32)],
    )
    slab = exchange(slab)
    read, new_state = call(
        functools.partial(state_kernel, parts=parts, tiles=tiles),
        (shape((parts, SLOTS // 2, HEAD_DIM), F32), shape((heads, HEAD_DIM, HEAD_DIM), F32)),
        (place, slab, old_state[0], retain, strength, head_gain.reshape(1, HEAD_DIM)),
        scratch=[pltpu.VMEM((parts, SLOTS, HEAD_DIM), F32)],
        spaces=[smem] + [vmem] * 5,
    )
    read = exchange(read)
    part = call(
        functools.partial(output_kernel, parts=parts, tiles=tiles),
        shape((parts, rows, width), BF16),
        (read, w_output),
    )
    part = exchange(part)
    hidden, residual = call(
        functools.partial(mixer_kernel, parts=parts),
        (shape((parts, rows, units), BF16), shape((parts, rows, share), BF16)),
        (part, x, channel_gain.reshape(1, width), w_gate.T, w_up.T),
    )
    hidden = exchange(hidden)
    mixed = call(
        functools.partial(down_kernel, parts=parts),
        shape((rows, share), BF16),
        (place, hidden, residual, w_down),
        spaces=[smem] + [vmem] * 3,
    )
    return mixed, new_state[None]


def body(
    tokens, old_state, mixer_gain, w_query, w_key, w_value, w_outgate, w_decay, w_write,
    decay_log, decay_bias, head_gain, w_output, channel_gain, w_gate, w_up, w_down, *, parts,
):
    rows, share = tokens.shape
    width = share * parts
    local_rows, heads = old_state.shape[:2]
    head_cols = w_query.shape[1]
    place = lax.axis_index("kv")

    tok_wide = gather_kv(tokens, parts).transpose(1, 0, 2).reshape(rows, width).astype(F32)
    scale_in = norm_scale(tok_wide)
    normed = (tok_wide * mixer_gain).astype(BF16)

    def project(weight):
        return (jnp.dot(normed, weight, preferred_element_type=F32) * scale_in).astype(BF16)

    packed = jnp.stack([project(w) for w in (w_query, w_key, w_value, w_outgate)], axis=1)
    packed = exchange(packed.reshape(parts, local_rows, 4, head_cols))

    own_normed = lax.dynamic_slice_in_dim(normed, place * local_rows, local_rows, 0)
    own_scale = lax.dynamic_slice_in_dim(scale_in, place * local_rows, local_rows, 0)
    decay_pre = jnp.dot(own_normed, w_decay, preferred_element_type=F32) * own_scale
    write_pre = jnp.dot(own_normed, w_write, preferred_element_type=F32) * own_scale

    def by_head(index):
        chosen = packed[:, :, index].transpose(1, 0, 2)
        return chosen.reshape(local_rows, heads, HEAD_DIM).astype(F32)

    queries = unit_rows(jax.nn.silu(by_head(0))) * HEAD_DIM ** (-0.5)
    keys_unit = unit_rows(jax.nn.silu(by_head(1)))
    values_act = jax.nn.silu(by_head(2))
    strength = jax.nn.sigmoid(write_pre)
    retain = jnp.exp(-jnp.exp(decay_log) * jax.nn.softplus(decay_pre + decay_bias))
    recalled = jnp.einsum("bhkv,bhk->bhv", old_state, keys_unit, precision=lax.Precision.HIGHEST)
    correction = values_act - retain[..., None] * recalled
    new_state = (
        retain[..., None, None] * old_state
        + (strength[..., None] * keys_unit)[..., :, None] * correction[..., None, :]
    )
    readout = jnp.einsum("bhkv,bhk->bhv", new_state, queries, precision=lax.Precision.HIGHEST)
    gated_read = readout * norm_scale(readout) * head_gain * jax.nn.silu(by_head(3))
    gated_read = gated_read.reshape(local_rows, parts, head_cols).astype(BF16)
    read_cols = exchange(gated_read.transpose(1, 0, 2)).reshape(rows, head_cols)

    partial_out = jnp.dot(read_cols, w_output, preferred_element_type=F32)
    mixer_out = exchange(partial_out.reshape(rows, parts, share).transpose(1, 0, 2)).sum(0)
    own_residual = (tokens.astype(F32) + mixer_out).astype(BF16)
    residual = gather_kv(own_residual, parts).transpose(1, 0, 2).reshape(rows, width)
    residual_wide = residual.astype(F32)
    scale_mid = norm_scale(residual_wide)
    normed_mid = (residual_wide * channel_gain).astype(BF16)
    gate_act = jnp.dot(normed_mid, w_gate, preferred_element_type=F32) * scale_mid
    upward = jnp.dot(normed_mid, w_up, preferred_element_type=F32) * scale_mid
    hidden = (jax.nn.silu(gate_act) * upward).astype(BF16)
    hidden = gather_kv(hidden, parts).transpose(1, 0, 2).reshape(rows, -1)
    down_sum = jnp.dot(hidden, w_down, preferred_element_type=F32)
    mixed = (own_residual.astype(F32) + down_sum).astype(BF16)
    return (mixed, new_state)


def solution(mesh):
    parts = mesh.shape["kv"]
    rows, states = P(("tp", "dp"), "kv"), P(("tp", "dp", "kv"), None, None, None)
    cols = P(None, "kv")
    in_specs = (rows, states, P(), cols, cols, cols, cols, P(), P(), P(), P(), P())
    in_specs += (P("kv", None), P(), cols, cols, cols)

    def step(*args):
        tokens, old_state = args[:2]
        share = tokens.shape[1]
        fits = (
            share % HEAD_DIM == 0
            and 4 * (share // HEAD_DIM) <= SLOTS
            and 3 * (share // HEAD_DIM) >= SLOTS // 2
            and old_state.shape[0] == 1
            and tokens.shape[0] == parts == 8
            and args[3].shape[1] == share
            and args[14].shape[1] % 16 == 0
        )
        return (fast_body if fits else body)(*args, parts=parts)

    return jax.shard_map(
        step, mesh=mesh, in_specs=in_specs, out_specs=(rows, states), check_vma=False
    )
```

```python
import functools

import jax
import jax.numpy as jnp
from jax import lax
from jax.experimental import pallas as pl
from jax.experimental.pallas import tpu as pltpu
from jax.sharding import PartitionSpec as P

HEAD_DIM = 128
EPS = 1e-06
MIB = 1 << 20

F32, BF16 = jnp.float32, jnp.bfloat16


def norm_scale(values):
    return lax.rsqrt(jnp.mean(values * values, axis=-1, keepdims=True) + EPS)


def unit_rows(values):
    return values * lax.rsqrt(jnp.sum(values * values, axis=-1, keepdims=True) + EPS)


def silu(values):
    return values / (1.0 + jnp.exp(-values))


def exchange(slabs):
    return lax.all_to_all(slabs, "kv", split_axis=0, concat_axis=0, tiled=True)


def gather_kv(block, parts):
    return exchange(jnp.broadcast_to(block[None], (parts,) + block.shape))


def call(kernel, out_shape, args, *, limit=8, scratch=(), spaces=None, outs=None, span=8):
    vmem = pl.BlockSpec(memory_space=pltpu.VMEM)
    specs = [vmem] * len(args) if spaces is None else spaces
    many = isinstance(out_shape, (tuple, list))
    return pl.pallas_call(
        kernel,
        out_shape=out_shape,
        in_specs=specs,
        out_specs=outs or ([vmem] * len(out_shape) if many else vmem),
        scratch_shapes=list(scratch),
        compiler_params=pltpu.CompilerParams(vmem_limit_bytes=limit * MIB),
        cost_estimate=pl.CostEstimate(
            flops=span * 500_000_000, bytes_accessed=span * 3_000_000, transcendentals=0
        ),
    )(*args)


def eye(n):
    across = lax.broadcasted_iota(jnp.int32, (n, n), 1)
    return lax.broadcasted_iota(jnp.int32, (n, n), 0) == across


def upright(row):
    return jnp.sum(jnp.where(eye(row.shape[1]), row, 0.0), axis=1, keepdims=True)


def pack_kernel(tok_ref, s_hbm, out_ref, buf, sems, *, parts, tiles):
    copies = [
        pltpu.make_async_copy(
            s_hbm.at[pl.ds(d * tiles, tiles)], buf.at[pl.ds(d * tiles, tiles)], sems.at[d]
        )
        for d in range(parts)
    ]
    for copy in copies:
        copy.start()
    depth = tiles * HEAD_DIM
    tok = tok_ref[...].astype(F32)
    tok = jnp.concatenate(
        [tok[:, t * HEAD_DIM : (t + 1) * HEAD_DIM] for t in range(tiles)], axis=0
    ).astype(BF16)
    for d in range(parts):
        out_ref[d, depth:, :] = tok
    for d, copy in enumerate(copies):
        copy.wait()
        for t in range(tiles):
            out_ref[d, t * HEAD_DIM : (t + 1) * HEAD_DIM, :] = buf[d * tiles + t].astype(BF16)


def eye(n):
    across = lax.broadcasted_iota(jnp.int32, (n, n), 1)
    return lax.broadcasted_iota(jnp.int32, (n, n), 0) == across


def upright(row):
    return jnp.sum(jnp.where(eye(row.shape[1]), row, 0.0), axis=1, keepdims=True)


def wide_tokens(x_ref, *, parts, tiles):
    depth = tiles * HEAD_DIM
    rows = (x_ref.shape[1] - depth) // tiles
    pieces = []
    for s in range(parts):
        tok = x_ref[s, depth:, :].astype(F32)
        pieces += [tok[t * rows : (t + 1) * rows, :] for t in range(tiles)]
    return jnp.concatenate(pieces, axis=-1)


def heads_kernel(
    place_ref, x_ref, gain_ref, wq, wk, wv, wg, wd_ref, ww_ref, log_ref, bias_ref,
    head_gain_ref, wo_ref, out_ref, retain_ref, strength_ref, kv, *, parts, tiles,
):
    nt = (((1,), (1,)), ((), ()))
    place = place_ref[0]
    x = wide_tokens(x_ref, parts=parts, tiles=tiles)
    rows, width = x.shape
    scale = norm_scale(x)
    normed = (x * gain_ref[...]).astype(BF16)

    decay = lax.dot_general(normed, wd_ref[...], nt, preferred_element_type=F32) * scale
    write = lax.dot_general(normed, ww_ref[...], nt, preferred_element_type=F32) * scale
    pre = decay + bias_ref[...]
    soft = jnp.maximum(pre, 0.0) + jnp.log1p(jnp.exp(-jnp.abs(pre)))
    retain_all = jnp.exp(-jnp.exp(log_ref[...]) * soft)
    strength_all = 1.0 / (1.0 + jnp.exp(-write))
    retain_ref[...] = retain_all
    strength_ref[...] = strength_all
    head = lax.broadcasted_iota(jnp.int32, retain_all.shape, 1)

    def project(w):
        acc = jnp.dot(normed, w[...], preferred_element_type=F32) * scale
        return acc.astype(BF16).astype(F32)

    query_pre, key_pre, value_pre, gate_pre = project(wq), project(wk), project(wv), project(wg)
    row = lax.broadcasted_iota(jnp.int32, (rows, HEAD_DIM), 0)
    kv[2 * tiles :] = jnp.zeros((kv.shape[0] - 2 * tiles, rows, HEAD_DIM), F32)
    gated = []
    for t in range(tiles):
        lanes = slice(t * HEAD_DIM, (t + 1) * HEAD_DIM)
        kv[t] = key_pre[:, lanes]
        kv[tiles + t] = value_pre[:, lanes]
        query = unit_rows(silu(query_pre[:, lanes])) * HEAD_DIM ** (-0.5)
        key = unit_rows(silu(key_pre[:, lanes]))
        value = silu(value_pre[:, lanes])
        own = head == place * tiles + t
        retain = jnp.sum(jnp.where(own, retain_all, 0.0), axis=1, keepdims=True)
        strength = jnp.sum(jnp.where(own, strength_all, 0.0), axis=1, keepdims=True)
        stack = []
        for vector in (key, query):
            high = vector.astype(BF16).astype(F32)
            stack += [high, vector - high]
        stack = jnp.concatenate(stack, axis=0).astype(BF16)
        found = [jnp.zeros((rows, HEAD_DIM), F32)] * 2
        for r in range(rows):
            product = jnp.dot(
                stack, x_ref[r, t * HEAD_DIM : (t + 1) * HEAD_DIM, :], preferred_element_type=F32
            )
            for i in range(2):
                both = product[2 * i * rows : (2 * i + 1) * rows] + product[
                    (2 * i + 1) * rows : (2 * i + 2) * rows
                ]
                found[i] = jnp.where(row == r, both, found[i])
        correction = value - retain * found[0]
        along = jnp.sum(key * query, axis=-1, keepdims=True)
        readout = retain * found[1] + (strength * along) * correction
        gated.append(
            readout * norm_scale(readout) * head_gain_ref[...] * silu(gate_pre[:, lanes])
        )
    gated = jnp.concatenate(gated, axis=-1).astype(BF16)
    part = jnp.dot(gated, wo_ref[...], preferred_element_type=F32).astype(BF16)
    for d in range(parts):
        out_ref[d, :, :width] = part
        out_ref[d, :, width:] = kv[:, d, :].astype(BF16)


def mixer_kernel(
    place_ref, part_ref, x_ref, gain_ref, retain_ref, strength_ref, s_ref, wg_ref, wu_ref,
    hid_ref, res_ref, new_hbm, new, sems, *, parts, tiles,
):
    nt = (((1,), (1,)), ((), ()))
    place = place_ref[0]
    width = gain_ref.shape[1]
    share = width // parts
    pre = jnp.concatenate([part_ref[j, :, width:].astype(F32) for j in range(parts)], axis=0)
    act = silu(pre)
    columns = unit_rows(act).T
    retain = jnp.broadcast_to(upright(retain_ref[pl.ds(place, 1), :]), (parts * tiles, HEAD_DIM))
    strength = jnp.broadcast_to(
        upright(strength_ref[pl.ds(place, 1), :]), (parts * tiles, HEAD_DIM)
    )
    slots = part_ref.shape[1]
    copies = []
    for j in range(parts):
        for t in range(tiles):
            h = j * tiles + t
            base = j * slots + t
            key = columns[:, base : base + 1]
            value = act[base + tiles : base + tiles + 1, :]
            old = s_ref[h]
            keep = retain[h : h + 1, :]
            recalled = jnp.sum(old * key, axis=0, keepdims=True)
            correction = (value - keep * recalled) * strength[h : h + 1, :]
            new[h] = keep * old + key * correction
        copies.append(
            pltpu.make_async_copy(
                new.at[pl.ds(j * tiles, tiles)], new_hbm.at[pl.ds(j * tiles, tiles)], sems.at[j]
            )
        )
        copies[-1].start()

    total = part_ref[0, :, :width].astype(F32)
    for s in range(1, parts):
        total = total + part_ref[s, :, :width].astype(F32)
    residual = (wide_tokens(x_ref, parts=parts, tiles=tiles) + total).astype(BF16)
    for s in range(parts):
        res_ref[s] = residual[:, s * share : (s + 1) * share]
    wide = residual.astype(F32)
    scale = norm_scale(wide)
    normed = (wide * gain_ref[...]).astype(BF16)
    gate = lax.dot_general(normed, wg_ref[...], nt, preferred_element_type=F32) * scale
    up = lax.dot_general(normed, wu_ref[...], nt, preferred_element_type=F32) * scale
    hidden = (silu(gate) * up).astype(BF16)
    for s in range(parts):
        hid_ref[s] = hidden
    for copy in copies:
        copy.wait()


def down_kernel(place_ref, hid_ref, res_ref, w_ref, out_ref, *, parts):
    units = hid_ref.shape[2]
    total = res_ref[place_ref[0]].astype(F32)
    for s in range(parts):
        total = total + jnp.dot(
            hid_ref[s], w_ref[s * units : (s + 1) * units, :], preferred_element_type=F32
        )
    out_ref[...] = total.astype(BF16)


def fast_body(
    tokens, old_state, mixer_gain, w_query, w_key, w_value, w_outgate, w_decay, w_write,
    decay_log, decay_bias, head_gain, w_output, channel_gain, w_gate, w_up, w_down, *, parts,
):
    rows, share = tokens.shape
    width = share * parts
    heads = old_state.shape[1]
    tiles = share // HEAD_DIM
    units = w_gate.shape[1]
    shape = jax.ShapeDtypeStruct
    place = lax.axis_index("kv").astype(jnp.int32).reshape(1)
    smem = pl.BlockSpec(memory_space=pltpu.SMEM)
    vmem = pl.BlockSpec(memory_space=pltpu.VMEM)
    hbm = pl.BlockSpec(memory_space=pltpu.HBM)
    states = (heads, HEAD_DIM, HEAD_DIM)
    state = old_state[0]

    tokens, place = lax.optimization_barrier((tokens, place))
    slabs = call(
        functools.partial(pack_kernel, parts=parts, tiles=tiles),
        shape((parts, tiles * (HEAD_DIM + rows), HEAD_DIM), BF16),
        (tokens, state),
        scratch=[pltpu.VMEM(states, F32), pltpu.SemaphoreType.DMA((parts,))],
        spaces=[vmem, hbm],
    )
    x = exchange(slabs)
    part, retain, strength = call(
        functools.partial(heads_kernel, parts=parts, tiles=tiles),
        (
            shape((parts, rows, width + HEAD_DIM), BF16),
            shape((rows, heads), F32),
            shape((rows, heads), F32),
        ),
        (
            place, x, mixer_gain.reshape(1, width), w_query, w_key, w_value, w_outgate,
            w_decay.T, w_write.T, decay_log.reshape(1, heads), decay_bias.reshape(1, heads),
            head_gain.reshape(1, HEAD_DIM), w_output,
        ),
        scratch=[pltpu.VMEM((rows, rows, HEAD_DIM), F32)],
        spaces=[smem] + [vmem] * 12,
    )
    part = exchange(part)
    hidden, residual, new_state = call(
        functools.partial(mixer_kernel, parts=parts, tiles=tiles),
        (
            shape((parts, rows, units), BF16),
            shape((parts, rows, share), BF16),
            shape(states, F32),
        ),
        (
            place, part, x, channel_gain.reshape(1, width), retain, strength, state,
            w_gate.T, w_up.T,
        ),
        scratch=[pltpu.VMEM(states, F32), pltpu.SemaphoreType.DMA((parts,))],
        spaces=[smem] + [vmem] * 8,
        outs=[vmem, vmem, hbm],
    )
    hidden = exchange(hidden)
    mixed = call(
        functools.partial(down_kernel, parts=parts),
        shape((rows, share), BF16),
        (place, hidden, residual, w_down),
        spaces=[smem] + [vmem] * 3,
    )
    return mixed, new_state[None]


def body(
    tokens, old_state, mixer_gain, w_query, w_key, w_value, w_outgate, w_decay, w_write,
    decay_log, decay_bias, head_gain, w_output, channel_gain, w_gate, w_up, w_down, *, parts,
):
    rows, share = tokens.shape
    width = share * parts
    local_rows, heads = old_state.shape[:2]
    head_cols = w_query.shape[1]
    place = lax.axis_index("kv")

    tok_wide = gather_kv(tokens, parts).transpose(1, 0, 2).reshape(rows, width).astype(F32)
    scale_in = norm_scale(tok_wide)
    normed = (tok_wide * mixer_gain).astype(BF16)

    def project(weight):
        return (jnp.dot(normed, weight, preferred_element_type=F32) * scale_in).astype(BF16)

    packed = jnp.stack([project(w) for w in (w_query, w_key, w_value, w_outgate)], axis=1)
    packed = exchange(packed.reshape(parts, local_rows, 4, head_cols))

    own_normed = lax.dynamic_slice_in_dim(normed, place * local_rows, local_rows, 0)
    own_scale = lax.dynamic_slice_in_dim(scale_in, place * local_rows, local_rows, 0)
    decay_pre = jnp.dot(own_normed, w_decay, preferred_element_type=F32) * own_scale
    write_pre = jnp.dot(own_normed, w_write, preferred_element_type=F32) * own_scale

    def by_head(index):
        chosen = packed[:, :, index].transpose(1, 0, 2)
        return chosen.reshape(local_rows, heads, HEAD_DIM).astype(F32)

    queries = unit_rows(jax.nn.silu(by_head(0))) * HEAD_DIM ** (-0.5)
    keys_unit = unit_rows(jax.nn.silu(by_head(1)))
    values_act = jax.nn.silu(by_head(2))
    strength = jax.nn.sigmoid(write_pre)
    retain = jnp.exp(-jnp.exp(decay_log) * jax.nn.softplus(decay_pre + decay_bias))
    recalled = jnp.einsum("bhkv,bhk->bhv", old_state, keys_unit, precision=lax.Precision.HIGHEST)
    correction = values_act - retain[..., None] * recalled
    new_state = (
        retain[..., None, None] * old_state
        + (strength[..., None] * keys_unit)[..., :, None] * correction[..., None, :]
    )
    readout = jnp.einsum("bhkv,bhk->bhv", new_state, queries, precision=lax.Precision.HIGHEST)
    gated_read = readout * norm_scale(readout) * head_gain * jax.nn.silu(by_head(3))
    gated_read = gated_read.reshape(local_rows, parts, head_cols).astype(BF16)
    read_cols = exchange(gated_read.transpose(1, 0, 2)).reshape(rows, head_cols)

    partial_out = jnp.dot(read_cols, w_output, preferred_element_type=F32)
    mixer_out = exchange(partial_out.reshape(rows, parts, share).transpose(1, 0, 2)).sum(0)
    own_residual = (tokens.astype(F32) + mixer_out).astype(BF16)
    residual = gather_kv(own_residual, parts).transpose(1, 0, 2).reshape(rows, width)
    residual_wide = residual.astype(F32)
    scale_mid = norm_scale(residual_wide)
    normed_mid = (residual_wide * channel_gain).astype(BF16)
    gate_act = jnp.dot(normed_mid, w_gate, preferred_element_type=F32) * scale_mid
    upward = jnp.dot(normed_mid, w_up, preferred_element_type=F32) * scale_mid
    hidden = (jax.nn.silu(gate_act) * upward).astype(BF16)
    hidden = gather_kv(hidden, parts).transpose(1, 0, 2).reshape(rows, -1)
    down_sum = jnp.dot(hidden, w_down, preferred_element_type=F32)
    mixed = (own_residual.astype(F32) + down_sum).astype(BF16)
    return (mixed, new_state)


def solution(mesh):
    parts = mesh.shape["kv"]
    rows, states = P(("tp", "dp"), "kv"), P(("tp", "dp", "kv"), None, None, None)
    cols = P(None, "kv")
    in_specs = (rows, states, P(), cols, cols, cols, cols, P(), P(), P(), P(), P())
    in_specs += (P("kv", None), P(), cols, cols, cols)

    def step(*args):
        tokens, old_state = args[:2]
        share = tokens.shape[1]
        fits = (
            share % HEAD_DIM == 0
            and 2 * (share // HEAD_DIM) <= tokens.shape[0]
            and old_state.shape[0] == 1
            and tokens.shape[0] == parts == 8
            and args[3].shape[1] == share
            and args[14].shape[1] % 16 == 0
        )
        return (fast_body if fits else body)(*args, parts=parts)

    return jax.shard_map(
        step, mesh=mesh, in_specs=in_specs, out_specs=(rows, states), check_vma=False
    )
```

```python
import functools

import jax
import jax.numpy as jnp
from jax import lax
from jax.experimental import pallas as pl
from jax.experimental.pallas import tpu as pltpu
from jax.sharding import PartitionSpec as P

HEAD_DIM = 128
EPS = 1e-06
MIB = 1 << 20

F32, BF16 = jnp.float32, jnp.bfloat16
FAR_FIRST = (6, 7, 4, 5, 2, 3, 1)


def norm_scale(values):
    return lax.rsqrt(jnp.mean(values * values, axis=-1, keepdims=True) + EPS)


def unit_rows(values):
    return values * lax.rsqrt(jnp.sum(values * values, axis=-1, keepdims=True) + EPS)


def silu(values):
    return values / (1.0 + jnp.exp(-values))


def exchange(slabs):
    return lax.all_to_all(slabs, "kv", split_axis=0, concat_axis=0, tiled=True)


def gather_kv(block, parts):
    return exchange(jnp.broadcast_to(block[None], (parts,) + block.shape))


def call(kernel, out_shape, args, *, limit=8, scratch=(), spaces=None, outs=None, span=8):
    vmem = pl.BlockSpec(memory_space=pltpu.VMEM)
    specs = [vmem] * len(args) if spaces is None else spaces
    many = isinstance(out_shape, (tuple, list))
    return pl.pallas_call(
        kernel,
        out_shape=out_shape,
        in_specs=specs,
        out_specs=outs or ([vmem] * len(out_shape) if many else vmem),
        scratch_shapes=list(scratch),
        compiler_params=pltpu.CompilerParams(vmem_limit_bytes=limit * MIB),
        cost_estimate=pl.CostEstimate(
            flops=span * 500_000_000, bytes_accessed=span * 3_000_000, transcendentals=0
        ),
    )(*args)


def eye(n):
    across = lax.broadcasted_iota(jnp.int32, (n, n), 1)
    return lax.broadcasted_iota(jnp.int32, (n, n), 0) == across


def upright(row):
    return jnp.sum(jnp.where(eye(row.shape[1]), row, 0.0), axis=1, keepdims=True)


def pack_kernel(place_ref, tok_hbm, s_hbm, *refs, parts, tiles):
    outs, (buf, tok_buf, sems) = refs[:parts], refs[parts:]
    place = place_ref[0]
    depth = tiles * HEAD_DIM
    tok_copy = pltpu.make_async_copy(tok_hbm, tok_buf, sems.at[parts])
    tok_copy.start()
    copies = []
    for x in range(parts):
        first = (place ^ x) * tiles
        copies.append(
            pltpu.make_async_copy(s_hbm.at[pl.ds(first, tiles)], buf.at[x], sems.at[x])
        )
        copies[-1].start()
    tok_copy.wait()
    tok = tok_buf[...].astype(F32)
    tok = jnp.concatenate(
        [tok[:, t * HEAD_DIM : (t + 1) * HEAD_DIM] for t in range(tiles)], axis=0
    ).astype(BF16)
    for x in range(parts):
        outs[x][depth:, :] = tok
    for x in range(parts):
        copies[x].wait()
        for t in range(tiles):
            outs[x][t * HEAD_DIM : (t + 1) * HEAD_DIM, :] = buf[x, t].astype(BF16)


def heads_kernel(
    place_ref, gain_ref, wq, wk, wv, wg, wd_ref, ww_ref, log_ref, bias_ref,
    head_gain_ref, wo_ref, *refs, parts, tiles,
):
    slabs = refs[:parts]
    out_ref, tok_ref, retain_ref, strength_ref, kv, order = refs[parts:]
    nt = (((1,), (1,)), ((), ()))
    place = place_ref[0]
    depth = tiles * HEAD_DIM
    rows = (slabs[0].shape[0] - depth) // tiles
    for x, slab in enumerate(slabs):
        order[place ^ x] = slab[depth:, :].astype(F32)
    x = jnp.concatenate(
        [order[s, t * rows : (t + 1) * rows, :] for s in range(parts) for t in range(tiles)],
        axis=-1,
    )
    tok_ref[...] = x.astype(BF16)
    width = x.shape[1]
    scale = norm_scale(x)
    normed = (x * gain_ref[...]).astype(BF16)

    decay = lax.dot_general(normed, wd_ref[...], nt, preferred_element_type=F32) * scale
    write = lax.dot_general(normed, ww_ref[...], nt, preferred_element_type=F32) * scale
    pre = decay + bias_ref[...]
    soft = jnp.maximum(pre, 0.0) + jnp.log1p(jnp.exp(-jnp.abs(pre)))
    retain_all = jnp.exp(-jnp.exp(log_ref[...]) * soft)
    strength_all = 1.0 / (1.0 + jnp.exp(-write))
    retain_ref[...] = retain_all
    strength_ref[...] = strength_all
    head = lax.broadcasted_iota(jnp.int32, retain_all.shape, 1)

    def project(w):
        acc = jnp.dot(normed, w[...], preferred_element_type=F32) * scale
        return acc.astype(BF16).astype(F32)

    query_pre, key_pre, value_pre, gate_pre = project(wq), project(wk), project(wv), project(wg)
    row = lax.broadcasted_iota(jnp.int32, (rows, HEAD_DIM), 0)
    kv[2 * tiles :] = jnp.zeros((kv.shape[0] - 2 * tiles, rows, HEAD_DIM), F32)
    gated = []
    for t in range(tiles):
        lanes = slice(t * HEAD_DIM, (t + 1) * HEAD_DIM)
        kv[t] = key_pre[:, lanes]
        kv[tiles + t] = value_pre[:, lanes]
        query = unit_rows(silu(query_pre[:, lanes])) * HEAD_DIM ** (-0.5)
        key = unit_rows(silu(key_pre[:, lanes]))
        value = silu(value_pre[:, lanes])
        own = head == place * tiles + t
        retain = jnp.sum(jnp.where(own, retain_all, 0.0), axis=1, keepdims=True)
        strength = jnp.sum(jnp.where(own, strength_all, 0.0), axis=1, keepdims=True)
        stack = []
        for vector in (key, query):
            high = vector.astype(BF16).astype(F32)
            stack += [high, vector - high]
        stack = jnp.concatenate(stack, axis=0).astype(BF16)
        found = [jnp.zeros((rows, HEAD_DIM), F32)] * 2
        for x, slab in enumerate(slabs):
            product = jnp.dot(
                stack, slab[t * HEAD_DIM : (t + 1) * HEAD_DIM, :], preferred_element_type=F32
            )
            for i in range(2):
                both = product[2 * i * rows : (2 * i + 1) * rows] + product[
                    (2 * i + 1) * rows : (2 * i + 2) * rows
                ]
                found[i] = jnp.where(row == place ^ x, both, found[i])
        correction = value - retain * found[0]
        along = jnp.sum(key * query, axis=-1, keepdims=True)
        readout = retain * found[1] + (strength * along) * correction
        gated.append(
            readout * norm_scale(readout) * head_gain_ref[...] * silu(gate_pre[:, lanes])
        )
    gated = jnp.concatenate(gated, axis=-1).astype(BF16)
    part = jnp.dot(gated, wo_ref[...], preferred_element_type=F32).astype(BF16)
    for d in range(parts):
        out_ref[d, :, :width] = part
        out_ref[d, :, width:] = kv[:, d, :].astype(BF16)


def mixer_kernel(
    place_ref, part_ref, tok_ref, gain_ref, retain_ref, strength_ref, s_ref, wg_ref, wu_ref,
    hid_ref, res_ref, new_hbm, new, sems, *, parts, tiles,
):
    nt = (((1,), (1,)), ((), ()))
    place = place_ref[0]
    width = gain_ref.shape[1]
    share = width // parts
    pre = jnp.concatenate([part_ref[j, :, width:].astype(F32) for j in range(parts)], axis=0)
    act = silu(pre)
    columns = unit_rows(act).T
    retain = jnp.broadcast_to(upright(retain_ref[pl.ds(place, 1), :]), (parts * tiles, HEAD_DIM))
    strength = jnp.broadcast_to(
        upright(strength_ref[pl.ds(place, 1), :]), (parts * tiles, HEAD_DIM)
    )
    slots = part_ref.shape[1]
    copies = []
    for j in range(parts):
        for t in range(tiles):
            h = j * tiles + t
            base = j * slots + t
            key = columns[:, base : base + 1]
            value = act[base + tiles : base + tiles + 1, :]
            old = s_ref[h]
            keep = retain[h : h + 1, :]
            recalled = jnp.sum(old * key, axis=0, keepdims=True)
            correction = (value - keep * recalled) * strength[h : h + 1, :]
            new[h] = keep * old + key * correction
        copies.append(
            pltpu.make_async_copy(
                new.at[pl.ds(j * tiles, tiles)], new_hbm.at[pl.ds(j * tiles, tiles)], sems.at[j]
            )
        )
        copies[-1].start()

    total = part_ref[0, :, :width].astype(F32)
    for s in range(1, parts):
        total = total + part_ref[s, :, :width].astype(F32)
    residual = (tok_ref[...].astype(F32) + total).astype(BF16)
    for s in range(parts):
        res_ref[s] = residual[:, s * share : (s + 1) * share]
    wide = residual.astype(F32)
    scale = norm_scale(wide)
    normed = (wide * gain_ref[...]).astype(BF16)
    gate = lax.dot_general(normed, wg_ref[...], nt, preferred_element_type=F32) * scale
    up = lax.dot_general(normed, wu_ref[...], nt, preferred_element_type=F32) * scale
    hidden = (silu(gate) * up).astype(BF16)
    for s in range(parts):
        hid_ref[s] = hidden
    for copy in copies:
        copy.wait()


def down_kernel(place_ref, hid_ref, res_ref, w_ref, out_ref, *, parts):
    units = hid_ref.shape[2]
    total = res_ref[place_ref[0]].astype(F32)
    for s in range(parts):
        total = total + jnp.dot(
            hid_ref[s], w_ref[s * units : (s + 1) * units, :], preferred_element_type=F32
        )
    out_ref[...] = total.astype(BF16)


def fast_body(
    tokens, old_state, mixer_gain, w_query, w_key, w_value, w_outgate, w_decay, w_write,
    decay_log, decay_bias, head_gain, w_output, channel_gain, w_gate, w_up, w_down, *, parts,
):
    rows, share = tokens.shape
    width = share * parts
    heads = old_state.shape[1]
    tiles = share // HEAD_DIM
    units = w_gate.shape[1]
    shape = jax.ShapeDtypeStruct
    place = lax.axis_index("kv").astype(jnp.int32).reshape(1)
    smem = pl.BlockSpec(memory_space=pltpu.SMEM)
    vmem = pl.BlockSpec(memory_space=pltpu.VMEM)
    hbm = pl.BlockSpec(memory_space=pltpu.HBM)
    states = (heads, HEAD_DIM, HEAD_DIM)
    state = old_state[0]

    tokens, place = lax.optimization_barrier((tokens, place))
    slab = shape((tiles * (HEAD_DIM + rows), HEAD_DIM), BF16)
    sent = call(
        functools.partial(pack_kernel, parts=parts, tiles=tiles),
        [slab] * parts,
        (place, pltpu.with_memory_space_constraint(tokens, pltpu.HBM),
         pltpu.with_memory_space_constraint(state, pltpu.HBM)),
        scratch=[
            pltpu.VMEM((parts, tiles) + states[1:], F32),
            pltpu.VMEM((rows, share), BF16),
            pltpu.SemaphoreType.DMA((parts + 1,)),
        ],
        spaces=[smem, hbm, hbm],
        span=40,
    )
    slabs = list(sent)
    for x in FAR_FIRST:
        slabs[x] = lax.ppermute(sent[x], "kv", [(i, i ^ x) for i in range(parts)])
    part, wide, retain, strength = call(
        functools.partial(heads_kernel, parts=parts, tiles=tiles),
        (
            shape((parts, rows, width + HEAD_DIM), BF16),
            shape((rows, width), BF16),
            shape((rows, heads), F32),
            shape((rows, heads), F32),
        ),
        (
            place, mixer_gain.reshape(1, width), w_query, w_key, w_value, w_outgate,
            w_decay.T, w_write.T, decay_log.reshape(1, heads), decay_bias.reshape(1, heads),
            head_gain.reshape(1, HEAD_DIM), w_output, *slabs,
        ),
        scratch=[
            pltpu.VMEM((rows, rows, HEAD_DIM), F32),
            pltpu.VMEM((parts, tiles * rows, HEAD_DIM), F32),
        ],
        spaces=[smem] + [vmem] * (11 + parts),
    )
    part = exchange(part)
    hidden, residual, new_state = call(
        functools.partial(mixer_kernel, parts=parts, tiles=tiles),
        (
            shape((parts, rows, units), BF16),
            shape((parts, rows, share), BF16),
            shape(states, F32),
        ),
        (
            place, part, wide, channel_gain.reshape(1, width), retain, strength, state,
            w_gate.T, w_up.T,
        ),
        scratch=[pltpu.VMEM(states, F32), pltpu.SemaphoreType.DMA((parts,))],
        spaces=[smem] + [vmem] * 8,
        outs=[vmem, vmem, hbm],
    )
    hidden = exchange(hidden)
    mixed = call(
        functools.partial(down_kernel, parts=parts),
        shape((rows, share), BF16),
        (place, hidden, residual, w_down),
        spaces=[smem] + [vmem] * 3,
    )
    return mixed, new_state[None]


def body(
    tokens, old_state, mixer_gain, w_query, w_key, w_value, w_outgate, w_decay, w_write,
    decay_log, decay_bias, head_gain, w_output, channel_gain, w_gate, w_up, w_down, *, parts,
):
    rows, share = tokens.shape
    width = share * parts
    local_rows, heads = old_state.shape[:2]
    head_cols = w_query.shape[1]
    place = lax.axis_index("kv")

    tok_wide = gather_kv(tokens, parts).transpose(1, 0, 2).reshape(rows, width).astype(F32)
    scale_in = norm_scale(tok_wide)
    normed = (tok_wide * mixer_gain).astype(BF16)

    def project(weight):
        return (jnp.dot(normed, weight, preferred_element_type=F32) * scale_in).astype(BF16)

    packed = jnp.stack([project(w) for w in (w_query, w_key, w_value, w_outgate)], axis=1)
    packed = exchange(packed.reshape(parts, local_rows, 4, head_cols))

    own_normed = lax.dynamic_slice_in_dim(normed, place * local_rows, local_rows, 0)
    own_scale = lax.dynamic_slice_in_dim(scale_in, place * local_rows, local_rows, 0)
    decay_pre = jnp.dot(own_normed, w_decay, preferred_element_type=F32) * own_scale
    write_pre = jnp.dot(own_normed, w_write, preferred_element_type=F32) * own_scale

    def by_head(index):
        chosen = packed[:, :, index].transpose(1, 0, 2)
        return chosen.reshape(local_rows, heads, HEAD_DIM).astype(F32)

    queries = unit_rows(jax.nn.silu(by_head(0))) * HEAD_DIM ** (-0.5)
    keys_unit = unit_rows(jax.nn.silu(by_head(1)))
    values_act = jax.nn.silu(by_head(2))
    strength = jax.nn.sigmoid(write_pre)
    retain = jnp.exp(-jnp.exp(decay_log) * jax.nn.softplus(decay_pre + decay_bias))
    recalled = jnp.einsum("bhkv,bhk->bhv", old_state, keys_unit, precision=lax.Precision.HIGHEST)
    correction = values_act - retain[..., None] * recalled
    new_state = (
        retain[..., None, None] * old_state
        + (strength[..., None] * keys_unit)[..., :, None] * correction[..., None, :]
    )
    readout = jnp.einsum("bhkv,bhk->bhv", new_state, queries, precision=lax.Precision.HIGHEST)
    gated_read = readout * norm_scale(readout) * head_gain * jax.nn.silu(by_head(3))
    gated_read = gated_read.reshape(local_rows, parts, head_cols).astype(BF16)
    read_cols = exchange(gated_read.transpose(1, 0, 2)).reshape(rows, head_cols)

    partial_out = jnp.dot(read_cols, w_output, preferred_element_type=F32)
    mixer_out = exchange(partial_out.reshape(rows, parts, share).transpose(1, 0, 2)).sum(0)
    own_residual = (tokens.astype(F32) + mixer_out).astype(BF16)
    residual = gather_kv(own_residual, parts).transpose(1, 0, 2).reshape(rows, width)
    residual_wide = residual.astype(F32)
    scale_mid = norm_scale(residual_wide)
    normed_mid = (residual_wide * channel_gain).astype(BF16)
    gate_act = jnp.dot(normed_mid, w_gate, preferred_element_type=F32) * scale_mid
    upward = jnp.dot(normed_mid, w_up, preferred_element_type=F32) * scale_mid
    hidden = (jax.nn.silu(gate_act) * upward).astype(BF16)
    hidden = gather_kv(hidden, parts).transpose(1, 0, 2).reshape(rows, -1)
    down_sum = jnp.dot(hidden, w_down, preferred_element_type=F32)
    mixed = (own_residual.astype(F32) + down_sum).astype(BF16)
    return (mixed, new_state)


def solution(mesh):
    parts = mesh.shape["kv"]
    rows, states = P(("tp", "dp"), "kv"), P(("tp", "dp", "kv"), None, None, None)
    cols = P(None, "kv")
    in_specs = (rows, states, P(), cols, cols, cols, cols, P(), P(), P(), P(), P())
    in_specs += (P("kv", None), P(), cols, cols, cols)

    def step(*args):
        tokens, old_state = args[:2]
        share = tokens.shape[1]
        fits = (
            share % HEAD_DIM == 0
            and 2 * (share // HEAD_DIM) <= tokens.shape[0]
            and old_state.shape[0] == 1
            and tokens.shape[0] == parts == 8
            and args[3].shape[1] == share
            and args[14].shape[1] % 16 == 0
        )
        return (fast_body if fits else body)(*args, parts=parts)

    return jax.shard_map(
        step, mesh=mesh, in_specs=in_specs, out_specs=(rows, states), check_vma=False
    )
```

```python
import functools

import jax
import jax.numpy as jnp
from jax import lax
from jax.experimental import pallas as pl
from jax.experimental.pallas import tpu as pltpu
from jax.sharding import PartitionSpec as P

HEAD_DIM = 128
EPS = 1e-06
MIB = 1 << 20

F32, BF16 = jnp.float32, jnp.bfloat16
FAR_FIRST = (6, 7, 4, 5, 2, 3, 1)


def norm_scale(values):
    return lax.rsqrt(jnp.mean(values * values, axis=-1, keepdims=True) + EPS)


def unit_rows(values):
    return values * lax.rsqrt(jnp.sum(values * values, axis=-1, keepdims=True) + EPS)


def silu(values):
    return values / (1.0 + jnp.exp(-values))


def exchange(slabs):
    return lax.all_to_all(slabs, "kv", split_axis=0, concat_axis=0, tiled=True)


def gather_kv(block, parts):
    return exchange(jnp.broadcast_to(block[None], (parts,) + block.shape))


def call(kernel, out_shape, args, *, limit=8, scratch=(), spaces=None, outs=None, span=8):
    vmem = pl.BlockSpec(memory_space=pltpu.VMEM)
    specs = [vmem] * len(args) if spaces is None else spaces
    many = isinstance(out_shape, (tuple, list))
    return pl.pallas_call(
        kernel,
        out_shape=out_shape,
        in_specs=specs,
        out_specs=outs or ([vmem] * len(out_shape) if many else vmem),
        scratch_shapes=list(scratch),
        compiler_params=pltpu.CompilerParams(vmem_limit_bytes=limit * MIB),
        cost_estimate=pl.CostEstimate(
            flops=span * 500_000_000, bytes_accessed=span * 3_000_000, transcendentals=0
        ),
    )(*args)


def eye(n):
    across = lax.broadcasted_iota(jnp.int32, (n, n), 1)
    return lax.broadcasted_iota(jnp.int32, (n, n), 0) == across


def upright(row):
    return jnp.sum(jnp.where(eye(row.shape[1]), row, 0.0), axis=1, keepdims=True)


def pack_kernel(place_ref, tok_hbm, s_hbm, *refs, parts, tiles):
    outs, (buf, tok_buf, sems) = refs[:parts], refs[parts:]
    place = place_ref[0]
    depth = tiles * HEAD_DIM
    tok_copy = pltpu.make_async_copy(tok_hbm, tok_buf, sems.at[parts])
    tok_copy.start()
    copies = []
    for x in range(parts):
        first = (place ^ x) * tiles
        copies.append(
            pltpu.make_async_copy(s_hbm.at[pl.ds(first, tiles)], buf.at[x], sems.at[x])
        )
        copies[-1].start()
    tok_copy.wait()
    tok = tok_buf[...].astype(F32)
    tok = jnp.concatenate(
        [tok[:, t * HEAD_DIM : (t + 1) * HEAD_DIM] for t in range(tiles)], axis=0
    ).astype(BF16)
    for x in range(parts):
        outs[x][depth:, :] = tok
    for x in range(parts):
        copies[x].wait()
        for t in range(tiles):
            outs[x][t * HEAD_DIM : (t + 1) * HEAD_DIM, :] = buf[x, t].astype(BF16)


def turn_kernel(after_ref, wg_hbm, wu_hbm, wg_ref, wu_ref, buf, sems):
    del after_ref
    units = wg_hbm.shape[0]
    cuts = [(a, min(a + HEAD_DIM, units)) for a in range(0, units, HEAD_DIM)]
    jobs = [(i, a, b) for i in range(2) for a, b in cuts]
    copies = [
        pltpu.make_async_copy(
            (wg_hbm, wu_hbm)[i].at[pl.ds(a, b - a)], buf.at[i, pl.ds(a, b - a)], sems.at[n]
        )
        for n, (i, a, b) in enumerate(jobs)
    ]
    for copy in copies:
        copy.start()
    for copy, (i, a, b) in zip(copies, jobs):
        copy.wait()
        (wg_ref, wu_ref)[i][:, a:b] = buf[i, a:b, :].T


def heads_kernel(
    place_ref, gain_ref, wq, wk, wv, wg, wd_ref, ww_ref, log_ref, bias_ref,
    head_gain_ref, wo_ref, *refs, parts, tiles,
):
    slabs = refs[:parts]
    out_ref, tok_ref, retain_ref, strength_ref, kv, order = refs[parts:]
    nt = (((1,), (1,)), ((), ()))
    place = place_ref[0]
    depth = tiles * HEAD_DIM
    rows = (slabs[0].shape[0] - depth) // tiles
    for x, slab in enumerate(slabs):
        order[place ^ x] = slab[depth:, :].astype(F32)
    x = jnp.concatenate(
        [order[s, t * rows : (t + 1) * rows, :] for s in range(parts) for t in range(tiles)],
        axis=-1,
    )
    tok_ref[...] = x.astype(BF16)
    width = x.shape[1]
    scale = norm_scale(x)
    normed = (x * gain_ref[...]).astype(BF16)

    decay = lax.dot_general(normed, wd_ref[...], nt, preferred_element_type=F32) * scale
    write = lax.dot_general(normed, ww_ref[...], nt, preferred_element_type=F32) * scale
    pre = decay + bias_ref[...]
    soft = jnp.maximum(pre, 0.0) + jnp.log1p(jnp.exp(-jnp.abs(pre)))
    retain_all = jnp.exp(-jnp.exp(log_ref[...]) * soft)
    strength_all = 1.0 / (1.0 + jnp.exp(-write))
    retain_ref[...] = retain_all
    strength_ref[...] = strength_all
    head = lax.broadcasted_iota(jnp.int32, retain_all.shape, 1)

    def project(w):
        acc = jnp.dot(normed, w[...], preferred_element_type=F32) * scale
        return acc.astype(BF16).astype(F32)

    query_pre, key_pre, value_pre, gate_pre = project(wq), project(wk), project(wv), project(wg)
    row = lax.broadcasted_iota(jnp.int32, (rows, HEAD_DIM), 0)
    kv[2 * tiles :] = jnp.zeros((kv.shape[0] - 2 * tiles, rows, HEAD_DIM), F32)
    gated = []
    for t in range(tiles):
        lanes = slice(t * HEAD_DIM, (t + 1) * HEAD_DIM)
        kv[t] = key_pre[:, lanes]
        kv[tiles + t] = value_pre[:, lanes]
        query = unit_rows(silu(query_pre[:, lanes])) * HEAD_DIM ** (-0.5)
        key = unit_rows(silu(key_pre[:, lanes]))
        value = silu(value_pre[:, lanes])
        own = head == place * tiles + t
        retain = jnp.sum(jnp.where(own, retain_all, 0.0), axis=1, keepdims=True)
        strength = jnp.sum(jnp.where(own, strength_all, 0.0), axis=1, keepdims=True)
        stack = []
        for vector in (key, query):
            high = vector.astype(BF16).astype(F32)
            stack += [high, vector - high]
        stack = jnp.concatenate(stack, axis=0).astype(BF16)
        found = [jnp.zeros((rows, HEAD_DIM), F32)] * 2
        for x, slab in enumerate(slabs):
            product = jnp.dot(
                stack, slab[t * HEAD_DIM : (t + 1) * HEAD_DIM, :], preferred_element_type=F32
            )
            for i in range(2):
                both = product[2 * i * rows : (2 * i + 1) * rows] + product[
                    (2 * i + 1) * rows : (2 * i + 2) * rows
                ]
                found[i] = jnp.where(row == place ^ x, both, found[i])
        correction = value - retain * found[0]
        along = jnp.sum(key * query, axis=-1, keepdims=True)
        readout = retain * found[1] + (strength * along) * correction
        gated.append(
            readout * norm_scale(readout) * head_gain_ref[...] * silu(gate_pre[:, lanes])
        )
    gated = jnp.concatenate(gated, axis=-1).astype(BF16)
    part = jnp.dot(gated, wo_ref[...], preferred_element_type=F32).astype(BF16)
    for d in range(parts):
        out_ref[d, :, :width] = part
        out_ref[d, :, width:] = kv[:, d, :].astype(BF16)


def mixer_kernel(
    place_ref, part_ref, tok_ref, gain_ref, retain_ref, strength_ref, s_ref, wg_ref, wu_ref,
    hid_ref, res_ref, new_hbm, new, sems, *, parts, tiles,
):
    place = place_ref[0]
    width = gain_ref.shape[1]
    share = width // parts
    pre = jnp.concatenate([part_ref[j, :, width:].astype(F32) for j in range(parts)], axis=0)
    act = silu(pre)
    columns = unit_rows(act).T
    retain = jnp.broadcast_to(upright(retain_ref[pl.ds(place, 1), :]), (parts * tiles, HEAD_DIM))
    strength = jnp.broadcast_to(
        upright(strength_ref[pl.ds(place, 1), :]), (parts * tiles, HEAD_DIM)
    )
    slots = part_ref.shape[1]
    copies = []
    for j in range(parts):
        for t in range(tiles):
            h = j * tiles + t
            base = j * slots + t
            key = columns[:, base : base + 1]
            value = act[base + tiles : base + tiles + 1, :]
            old = s_ref[h]
            keep = retain[h : h + 1, :]
            recalled = jnp.sum(old * key, axis=0, keepdims=True)
            correction = (value - keep * recalled) * strength[h : h + 1, :]
            new[h] = keep * old + key * correction
        copies.append(
            pltpu.make_async_copy(
                new.at[pl.ds(j * tiles, tiles)], new_hbm.at[pl.ds(j * tiles, tiles)], sems.at[j]
            )
        )
        copies[-1].start()

    total = part_ref[0, :, :width].astype(F32)
    for s in range(1, parts):
        total = total + part_ref[s, :, :width].astype(F32)
    residual = (tok_ref[...].astype(F32) + total).astype(BF16)
    for s in range(parts):
        res_ref[s] = residual[:, s * share : (s + 1) * share]
    wide = residual.astype(F32)
    scale = norm_scale(wide)
    normed = (wide * gain_ref[...]).astype(BF16)
    gate = jnp.dot(normed, wg_ref[...], preferred_element_type=F32) * scale
    up = jnp.dot(normed, wu_ref[...], preferred_element_type=F32) * scale
    hidden = (silu(gate) * up).astype(BF16)
    for s in range(parts):
        hid_ref[s] = hidden
    for copy in copies:
        copy.wait()


def down_kernel(place_ref, hid_ref, res_ref, w_ref, out_ref, *, parts):
    units = hid_ref.shape[2]
    total = res_ref[place_ref[0]].astype(F32)
    for s in range(parts):
        total = total + jnp.dot(
            hid_ref[s], w_ref[s * units : (s + 1) * units, :], preferred_element_type=F32
        )
    out_ref[...] = total.astype(BF16)


def fast_body(
    tokens, old_state, mixer_gain, w_query, w_key, w_value, w_outgate, w_decay, w_write,
    decay_log, decay_bias, head_gain, w_output, channel_gain, w_gate, w_up, w_down, *, parts,
):
    rows, share = tokens.shape
    width = share * parts
    heads = old_state.shape[1]
    tiles = share // HEAD_DIM
    units = w_gate.shape[1]
    shape = jax.ShapeDtypeStruct
    place = lax.axis_index("kv").astype(jnp.int32).reshape(1)
    smem = pl.BlockSpec(memory_space=pltpu.SMEM)
    vmem = pl.BlockSpec(memory_space=pltpu.VMEM)
    hbm = pl.BlockSpec(memory_space=pltpu.HBM)
    states = (heads, HEAD_DIM, HEAD_DIM)
    state = old_state[0]

    tokens, place = lax.optimization_barrier((tokens, place))
    slab = shape((tiles * (HEAD_DIM + rows), HEAD_DIM), BF16)
    sent = call(
        functools.partial(pack_kernel, parts=parts, tiles=tiles),
        [slab] * parts,
        (place, pltpu.with_memory_space_constraint(tokens, pltpu.HBM),
         pltpu.with_memory_space_constraint(state, pltpu.HBM)),
        scratch=[
            pltpu.VMEM((parts, tiles) + states[1:], F32),
            pltpu.VMEM((rows, share), BF16),
            pltpu.SemaphoreType.DMA((parts + 1,)),
        ],
        spaces=[smem, hbm, hbm],
        span=1,
    )
    slabs = list(sent)
    for x in FAR_FIRST:
        slabs[x] = lax.ppermute(sent[x], "kv", [(i, i ^ x) for i in range(parts)])
    turned = shape((width, units), BF16)
    wide_gate, wide_up = call(
        turn_kernel,
        (turned, turned),
        (sent[0], pltpu.with_memory_space_constraint(w_gate.T, pltpu.HBM),
         pltpu.with_memory_space_constraint(w_up.T, pltpu.HBM)),
        scratch=[
            pltpu.VMEM((2, units, width), BF16),
            pltpu.SemaphoreType.DMA((2 * pl.cdiv(units, HEAD_DIM),)),
        ],
        spaces=[vmem, hbm, hbm],
        limit=16,
        span=40,
    )
    slabs, wide_gate, wide_up = lax.optimization_barrier((slabs, wide_gate, wide_up))
    part, wide, retain, strength = call(
        functools.partial(heads_kernel, parts=parts, tiles=tiles),
        (
            shape((parts, rows, width + HEAD_DIM), BF16),
            shape((rows, width), BF16),
            shape((rows, heads), F32),
            shape((rows, heads), F32),
        ),
        (
            place, mixer_gain.reshape(1, width), w_query, w_key, w_value, w_outgate,
            w_decay.T, w_write.T, decay_log.reshape(1, heads), decay_bias.reshape(1, heads),
            head_gain.reshape(1, HEAD_DIM), w_output, *slabs,
        ),
        scratch=[
            pltpu.VMEM((rows, rows, HEAD_DIM), F32),
            pltpu.VMEM((parts, tiles * rows, HEAD_DIM), F32),
        ],
        spaces=[smem] + [vmem] * (11 + parts),
    )
    part = exchange(part)
    hidden, residual, new_state = call(
        functools.partial(mixer_kernel, parts=parts, tiles=tiles),
        (
            shape((parts, rows, units), BF16),
            shape((parts, rows, share), BF16),
            shape(states, F32),
        ),
        (
            place, part, wide, channel_gain.reshape(1, width), retain, strength, state,
            wide_gate, wide_up,
        ),
        scratch=[pltpu.VMEM(states, F32), pltpu.SemaphoreType.DMA((parts,))],
        spaces=[smem] + [vmem] * 8,
        outs=[vmem, vmem, hbm],
    )
    hidden = exchange(hidden)
    mixed = call(
        functools.partial(down_kernel, parts=parts),
        shape((rows, share), BF16),
        (place, hidden, residual, w_down),
        spaces=[smem] + [vmem] * 3,
    )
    return mixed, new_state[None]


def body(
    tokens, old_state, mixer_gain, w_query, w_key, w_value, w_outgate, w_decay, w_write,
    decay_log, decay_bias, head_gain, w_output, channel_gain, w_gate, w_up, w_down, *, parts,
):
    rows, share = tokens.shape
    width = share * parts
    local_rows, heads = old_state.shape[:2]
    head_cols = w_query.shape[1]
    place = lax.axis_index("kv")

    tok_wide = gather_kv(tokens, parts).transpose(1, 0, 2).reshape(rows, width).astype(F32)
    scale_in = norm_scale(tok_wide)
    normed = (tok_wide * mixer_gain).astype(BF16)

    def project(weight):
        return (jnp.dot(normed, weight, preferred_element_type=F32) * scale_in).astype(BF16)

    packed = jnp.stack([project(w) for w in (w_query, w_key, w_value, w_outgate)], axis=1)
    packed = exchange(packed.reshape(parts, local_rows, 4, head_cols))

    own_normed = lax.dynamic_slice_in_dim(normed, place * local_rows, local_rows, 0)
    own_scale = lax.dynamic_slice_in_dim(scale_in, place * local_rows, local_rows, 0)
    decay_pre = jnp.dot(own_normed, w_decay, preferred_element_type=F32) * own_scale
    write_pre = jnp.dot(own_normed, w_write, preferred_element_type=F32) * own_scale

    def by_head(index):
        chosen = packed[:, :, index].transpose(1, 0, 2)
        return chosen.reshape(local_rows, heads, HEAD_DIM).astype(F32)

    queries = unit_rows(jax.nn.silu(by_head(0))) * HEAD_DIM ** (-0.5)
    keys_unit = unit_rows(jax.nn.silu(by_head(1)))
    values_act = jax.nn.silu(by_head(2))
    strength = jax.nn.sigmoid(write_pre)
    retain = jnp.exp(-jnp.exp(decay_log) * jax.nn.softplus(decay_pre + decay_bias))
    recalled = jnp.einsum("bhkv,bhk->bhv", old_state, keys_unit, precision=lax.Precision.HIGHEST)
    correction = values_act - retain[..., None] * recalled
    new_state = (
        retain[..., None, None] * old_state
        + (strength[..., None] * keys_unit)[..., :, None] * correction[..., None, :]
    )
    readout = jnp.einsum("bhkv,bhk->bhv", new_state, queries, precision=lax.Precision.HIGHEST)
    gated_read = readout * norm_scale(readout) * head_gain * jax.nn.silu(by_head(3))
    gated_read = gated_read.reshape(local_rows, parts, head_cols).astype(BF16)
    read_cols = exchange(gated_read.transpose(1, 0, 2)).reshape(rows, head_cols)

    partial_out = jnp.dot(read_cols, w_output, preferred_element_type=F32)
    mixer_out = exchange(partial_out.reshape(rows, parts, share).transpose(1, 0, 2)).sum(0)
    own_residual = (tokens.astype(F32) + mixer_out).astype(BF16)
    residual = gather_kv(own_residual, parts).transpose(1, 0, 2).reshape(rows, width)
    residual_wide = residual.astype(F32)
    scale_mid = norm_scale(residual_wide)
    normed_mid = (residual_wide * channel_gain).astype(BF16)
    gate_act = jnp.dot(normed_mid, w_gate, preferred_element_type=F32) * scale_mid
    upward = jnp.dot(normed_mid, w_up, preferred_element_type=F32) * scale_mid
    hidden = (jax.nn.silu(gate_act) * upward).astype(BF16)
    hidden = gather_kv(hidden, parts).transpose(1, 0, 2).reshape(rows, -1)
    down_sum = jnp.dot(hidden, w_down, preferred_element_type=F32)
    mixed = (own_residual.astype(F32) + down_sum).astype(BF16)
    return (mixed, new_state)


def solution(mesh):
    parts = mesh.shape["kv"]
    rows, states = P(("tp", "dp"), "kv"), P(("tp", "dp", "kv"), None, None, None)
    cols = P(None, "kv")
    in_specs = (rows, states, P(), cols, cols, cols, cols, P(), P(), P(), P(), P())
    in_specs += (P("kv", None), P(), cols, cols, cols)

    def step(*args):
        tokens, old_state = args[:2]
        share = tokens.shape[1]
        fits = (
            share % HEAD_DIM == 0
            and 2 * (share // HEAD_DIM) <= tokens.shape[0]
            and old_state.shape[0] == 1
            and tokens.shape[0] == parts == 8
            and args[3].shape[1] == share
            and args[14].shape[1] % 16 == 0
        )
        return (fast_body if fits else body)(*args, parts=parts)

    return jax.shard_map(
        step, mesh=mesh, in_specs=in_specs, out_specs=(rows, states), check_vma=False
    )
```

```python
import functools

import jax
import jax.numpy as jnp
from jax import lax
from jax.experimental import pallas as pl
from jax.experimental.pallas import tpu as pltpu
from jax.sharding import PartitionSpec as P

HEAD_DIM = 128
EPS = 1e-06
MIB = 1 << 20

F32, BF16 = jnp.float32, jnp.bfloat16
FAR_FIRST = (6, 7, 4, 5, 2, 3, 1)


def norm_scale(values):
    return lax.rsqrt(jnp.mean(values * values, axis=-1, keepdims=True) + EPS)


def unit_rows(values):
    return values * lax.rsqrt(jnp.sum(values * values, axis=-1, keepdims=True) + EPS)


def silu(values):
    return values / (1.0 + jnp.exp(-values))


def exchange(slabs):
    return lax.all_to_all(slabs, "kv", split_axis=0, concat_axis=0, tiled=True)


def swap(sent):
    got = list(sent)
    for x in FAR_FIRST:
        got[x] = lax.ppermute(sent[x], "kv", [(i, i ^ x) for i in range(len(sent))])
    return got


def gather_kv(block, parts):
    return exchange(jnp.broadcast_to(block[None], (parts,) + block.shape))


def call(kernel, out_shape, args, *, limit=8, scratch=(), spaces=None, outs=None, span=8):
    vmem = pl.BlockSpec(memory_space=pltpu.VMEM)
    specs = [vmem] * len(args) if spaces is None else spaces
    many = isinstance(out_shape, (tuple, list))
    return pl.pallas_call(
        kernel,
        out_shape=out_shape,
        in_specs=specs,
        out_specs=outs or ([vmem] * len(out_shape) if many else vmem),
        scratch_shapes=list(scratch),
        compiler_params=pltpu.CompilerParams(vmem_limit_bytes=limit * MIB),
        cost_estimate=pl.CostEstimate(
            flops=span * 500_000_000, bytes_accessed=span * 3_000_000, transcendentals=0
        ),
    )(*args)


def eye(n):
    across = lax.broadcasted_iota(jnp.int32, (n, n), 1)
    return lax.broadcasted_iota(jnp.int32, (n, n), 0) == across


def upright(row):
    return jnp.sum(jnp.where(eye(row.shape[1]), row, 0.0), axis=1, keepdims=True)


def pack_kernel(place_ref, tok_hbm, s_hbm, *refs, parts, tiles):
    outs, (buf, tok_buf, sems) = refs[:parts], refs[parts:]
    place = place_ref[0]
    depth = tiles * HEAD_DIM
    tok_copy = pltpu.make_async_copy(tok_hbm, tok_buf, sems.at[parts])
    tok_copy.start()
    copies = []
    for x in range(parts):
        first = (place ^ x) * tiles
        copies.append(
            pltpu.make_async_copy(s_hbm.at[pl.ds(first, tiles)], buf.at[x], sems.at[x])
        )
        copies[-1].start()
    tok_copy.wait()
    tok = tok_buf[...].astype(F32)
    tok = jnp.concatenate(
        [tok[:, t * HEAD_DIM : (t + 1) * HEAD_DIM] for t in range(tiles)], axis=0
    ).astype(BF16)
    for x in range(parts):
        outs[x][depth:, :] = tok
    for x in range(parts):
        copies[x].wait()
        for t in range(tiles):
            outs[x][t * HEAD_DIM : (t + 1) * HEAD_DIM, :] = buf[x, t].astype(BF16)


def turn_kernel(after_ref, wg_hbm, wu_hbm, wg_ref, wu_ref, buf, sems):
    del after_ref
    units = wg_hbm.shape[0]
    cuts = [(a, min(a + HEAD_DIM, units)) for a in range(0, units, HEAD_DIM)]
    jobs = [(i, a, b) for i in range(2) for a, b in cuts]
    copies = [
        pltpu.make_async_copy(
            (wg_hbm, wu_hbm)[i].at[pl.ds(a, b - a)], buf.at[i, pl.ds(a, b - a)], sems.at[n]
        )
        for n, (i, a, b) in enumerate(jobs)
    ]
    for copy in copies:
        copy.start()
    for copy, (i, a, b) in zip(copies, jobs):
        copy.wait()
        (wg_ref, wu_ref)[i][:, a:b] = buf[i, a:b, :].T


def heads_kernel(
    place_ref, gain_ref, wq, wk, wv, wg, wd_ref, ww_ref, log_ref, bias_ref,
    head_gain_ref, wo_ref, *refs, parts, tiles,
):
    slabs, outs = refs[:parts], refs[parts : 2 * parts]
    tok_ref, retain_ref, strength_ref, kv, order = refs[2 * parts :]
    nt = (((1,), (1,)), ((), ()))
    place = place_ref[0]
    depth = tiles * HEAD_DIM
    rows = (slabs[0].shape[0] - depth) // tiles
    for x, slab in enumerate(slabs):
        order[place ^ x] = slab[depth:, :].astype(F32)
    x = jnp.concatenate(
        [order[s, t * rows : (t + 1) * rows, :] for s in range(parts) for t in range(tiles)],
        axis=-1,
    )
    tok_ref[...] = x.astype(BF16)
    width = x.shape[1]
    scale = norm_scale(x)
    normed = (x * gain_ref[...]).astype(BF16)

    decay = lax.dot_general(normed, wd_ref[...], nt, preferred_element_type=F32) * scale
    write = lax.dot_general(normed, ww_ref[...], nt, preferred_element_type=F32) * scale
    pre = decay + bias_ref[...]
    soft = jnp.maximum(pre, 0.0) + jnp.log1p(jnp.exp(-jnp.abs(pre)))
    retain_all = jnp.exp(-jnp.exp(log_ref[...]) * soft)
    strength_all = 1.0 / (1.0 + jnp.exp(-write))
    retain_ref[...] = retain_all
    strength_ref[...] = strength_all
    head = lax.broadcasted_iota(jnp.int32, retain_all.shape, 1)

    def project(w):
        acc = jnp.dot(normed, w[...], preferred_element_type=F32) * scale
        return acc.astype(BF16).astype(F32)

    query_pre, key_pre, value_pre, gate_pre = project(wq), project(wk), project(wv), project(wg)
    row = lax.broadcasted_iota(jnp.int32, (rows, HEAD_DIM), 0)
    kv[:, 2 * tiles :, :] = jnp.zeros((rows, kv.shape[1] - 2 * tiles, HEAD_DIM), F32)
    gated = []
    for t in range(tiles):
        lanes = slice(t * HEAD_DIM, (t + 1) * HEAD_DIM)
        kv[:, t, :] = key_pre[:, lanes]
        kv[:, tiles + t, :] = value_pre[:, lanes]
        query = unit_rows(silu(query_pre[:, lanes])) * HEAD_DIM ** (-0.5)
        key = unit_rows(silu(key_pre[:, lanes]))
        value = silu(value_pre[:, lanes])
        own = head == place * tiles + t
        retain = jnp.sum(jnp.where(own, retain_all, 0.0), axis=1, keepdims=True)
        strength = jnp.sum(jnp.where(own, strength_all, 0.0), axis=1, keepdims=True)
        stack = []
        for vector in (key, query):
            high = vector.astype(BF16).astype(F32)
            stack += [high, vector - high]
        stack = jnp.concatenate(stack, axis=0).astype(BF16)
        found = [jnp.zeros((rows, HEAD_DIM), F32)] * 2
        for x, slab in enumerate(slabs):
            product = jnp.dot(
                stack, slab[t * HEAD_DIM : (t + 1) * HEAD_DIM, :], preferred_element_type=F32
            )
            for i in range(2):
                both = product[2 * i * rows : (2 * i + 1) * rows] + product[
                    (2 * i + 1) * rows : (2 * i + 2) * rows
                ]
                found[i] = jnp.where(row == place ^ x, both, found[i])
        correction = value - retain * found[0]
        along = jnp.sum(key * query, axis=-1, keepdims=True)
        readout = retain * found[1] + (strength * along) * correction
        gated.append(
            readout * norm_scale(readout) * head_gain_ref[...] * silu(gate_pre[:, lanes])
        )
    gated = jnp.concatenate(gated, axis=-1).astype(BF16)
    part = jnp.dot(gated, wo_ref[...], preferred_element_type=F32).astype(BF16)
    for x, out in enumerate(outs):
        out[:, :width] = part
        out[:, width:] = kv[place ^ x].astype(BF16)


def mixer_kernel(
    place_ref, tok_ref, gain_ref, retain_ref, strength_ref, s_ref, wg_ref, wu_ref, *refs,
    parts, tiles,
):
    partials = refs[:parts]
    hid_ref, res_ref, new_hbm, new, keep_rows, gain_rows, sems = refs[parts:]
    place = place_ref[0]
    width = gain_ref.shape[1]
    share = width // parts
    pre = jnp.concatenate([ref[:, width:].astype(F32) for ref in partials], axis=0)
    act = silu(pre)
    columns = unit_rows(act).T
    own = pl.ds(place, 1)
    keep_rows[...] = jnp.broadcast_to(upright(retain_ref[own, :]), keep_rows.shape)
    gain_rows[...] = jnp.broadcast_to(upright(strength_ref[own, :]), gain_rows.shape)
    slots = partials[0].shape[0]
    copies = []
    for x in range(parts):
        first = (place ^ x) * tiles
        for t in range(tiles):
            base = x * slots + t
            key = columns[:, base : base + 1]
            value = act[base + tiles : base + tiles + 1, :]
            old = s_ref[first + t]
            keep = keep_rows[pl.ds(first + t, 1), :]
            recalled = jnp.sum(old * key, axis=0, keepdims=True)
            correction = (value - keep * recalled) * gain_rows[pl.ds(first + t, 1), :]
            new[x, t] = keep * old + key * correction
        copies.append(
            pltpu.make_async_copy(new.at[x], new_hbm.at[pl.ds(first, tiles)], sems.at[x])
        )
        copies[-1].start()

    sums = [ref[:, :width].astype(F32) for ref in partials]
    while len(sums) > 1:
        sums = [a + b for a, b in zip(sums[::2], sums[1::2])]
    residual = (tok_ref[...].astype(F32) + sums[0]).astype(BF16)
    for s in range(parts):
        res_ref[s] = residual[:, s * share : (s + 1) * share]
    wide = residual.astype(F32)
    scale = norm_scale(wide)
    normed = (wide * gain_ref[...]).astype(BF16)
    gate = jnp.dot(normed, wg_ref[...], preferred_element_type=F32) * scale
    up = jnp.dot(normed, wu_ref[...], preferred_element_type=F32) * scale
    hidden = (silu(gate) * up).astype(BF16)
    for s in range(parts):
        hid_ref[s] = hidden
    for copy in copies:
        copy.wait()


def down_kernel(place_ref, hid_ref, res_ref, w_ref, out_ref, *, parts):
    units = hid_ref.shape[2]
    total = res_ref[place_ref[0]].astype(F32)
    for s in range(parts):
        total = total + jnp.dot(
            hid_ref[s], w_ref[s * units : (s + 1) * units, :], preferred_element_type=F32
        )
    out_ref[...] = total.astype(BF16)


def fast_body(
    tokens, old_state, mixer_gain, w_query, w_key, w_value, w_outgate, w_decay, w_write,
    decay_log, decay_bias, head_gain, w_output, channel_gain, w_gate, w_up, w_down, *, parts,
):
    rows, share = tokens.shape
    width = share * parts
    heads = old_state.shape[1]
    tiles = share // HEAD_DIM
    units = w_gate.shape[1]
    shape = jax.ShapeDtypeStruct
    place = lax.axis_index("kv").astype(jnp.int32).reshape(1)
    smem = pl.BlockSpec(memory_space=pltpu.SMEM)
    vmem = pl.BlockSpec(memory_space=pltpu.VMEM)
    hbm = pl.BlockSpec(memory_space=pltpu.HBM)
    states = (heads, HEAD_DIM, HEAD_DIM)
    state = old_state[0]

    tokens, place = lax.optimization_barrier((tokens, place))
    slab = shape((tiles * (HEAD_DIM + rows), HEAD_DIM), BF16)
    sent = call(
        functools.partial(pack_kernel, parts=parts, tiles=tiles),
        [slab] * parts,
        (place, pltpu.with_memory_space_constraint(tokens, pltpu.HBM),
         pltpu.with_memory_space_constraint(state, pltpu.HBM)),
        scratch=[
            pltpu.VMEM((parts, tiles) + states[1:], F32),
            pltpu.VMEM((rows, share), BF16),
            pltpu.SemaphoreType.DMA((parts + 1,)),
        ],
        spaces=[smem, hbm, hbm],
        span=1,
    )
    slabs = swap(sent)
    turned = shape((width, units), BF16)
    wide_gate, wide_up = call(
        turn_kernel,
        (turned, turned),
        (sent[0], pltpu.with_memory_space_constraint(w_gate.T, pltpu.HBM),
         pltpu.with_memory_space_constraint(w_up.T, pltpu.HBM)),
        scratch=[
            pltpu.VMEM((2, units, width), BF16),
            pltpu.SemaphoreType.DMA((2 * pl.cdiv(units, HEAD_DIM),)),
        ],
        spaces=[vmem, hbm, hbm],
        limit=16,
        span=40,
    )
    slabs, wide_gate, wide_up = lax.optimization_barrier((slabs, wide_gate, wide_up))
    *parted, wide, retain, strength = call(
        functools.partial(heads_kernel, parts=parts, tiles=tiles),
        (
            *[shape((rows, width + HEAD_DIM), BF16)] * parts,
            shape((rows, width), BF16),
            shape((rows, heads), F32),
            shape((rows, heads), F32),
        ),
        (
            place, mixer_gain.reshape(1, width), w_query, w_key, w_value, w_outgate,
            w_decay.T, w_write.T, decay_log.reshape(1, heads), decay_bias.reshape(1, heads),
            head_gain.reshape(1, HEAD_DIM), w_output, *slabs,
        ),
        scratch=[
            pltpu.VMEM((rows, rows, HEAD_DIM), F32),
            pltpu.VMEM((parts, tiles * rows, HEAD_DIM), F32),
        ],
        spaces=[smem] + [vmem] * (11 + parts),
    )
    parted = swap(parted)
    hidden, residual, new_state = call(
        functools.partial(mixer_kernel, parts=parts, tiles=tiles),
        (
            shape((parts, rows, units), BF16),
            shape((parts, rows, share), BF16),
            shape(states, F32),
        ),
        (
            place, wide, channel_gain.reshape(1, width), retain, strength, state,
            wide_gate, wide_up, *parted,
        ),
        scratch=[
            pltpu.VMEM((parts, tiles) + states[1:], F32),
            pltpu.VMEM((heads, HEAD_DIM), F32),
            pltpu.VMEM((heads, HEAD_DIM), F32),
            pltpu.SemaphoreType.DMA((parts,)),
        ],
        spaces=[smem] + [vmem] * (7 + parts),
        outs=[vmem, vmem, hbm],
    )
    hidden = exchange(hidden)
    mixed = call(
        functools.partial(down_kernel, parts=parts),
        shape((rows, share), BF16),
        (place, hidden, residual, w_down),
        spaces=[smem] + [vmem] * 3,
    )
    return mixed, new_state[None]


def body(
    tokens, old_state, mixer_gain, w_query, w_key, w_value, w_outgate, w_decay, w_write,
    decay_log, decay_bias, head_gain, w_output, channel_gain, w_gate, w_up, w_down, *, parts,
):
    rows, share = tokens.shape
    width = share * parts
    local_rows, heads = old_state.shape[:2]
    head_cols = w_query.shape[1]
    place = lax.axis_index("kv")

    tok_wide = gather_kv(tokens, parts).transpose(1, 0, 2).reshape(rows, width).astype(F32)
    scale_in = norm_scale(tok_wide)
    normed = (tok_wide * mixer_gain).astype(BF16)

    def project(weight):
        return (jnp.dot(normed, weight, preferred_element_type=F32) * scale_in).astype(BF16)

    packed = jnp.stack([project(w) for w in (w_query, w_key, w_value, w_outgate)], axis=1)
    packed = exchange(packed.reshape(parts, local_rows, 4, head_cols))

    own_normed = lax.dynamic_slice_in_dim(normed, place * local_rows, local_rows, 0)
    own_scale = lax.dynamic_slice_in_dim(scale_in, place * local_rows, local_rows, 0)
    decay_pre = jnp.dot(own_normed, w_decay, preferred_element_type=F32) * own_scale
    write_pre = jnp.dot(own_normed, w_write, preferred_element_type=F32) * own_scale

    def by_head(index):
        chosen = packed[:, :, index].transpose(1, 0, 2)
        return chosen.reshape(local_rows, heads, HEAD_DIM).astype(F32)

    queries = unit_rows(jax.nn.silu(by_head(0))) * HEAD_DIM ** (-0.5)
    keys_unit = unit_rows(jax.nn.silu(by_head(1)))
    values_act = jax.nn.silu(by_head(2))
    strength = jax.nn.sigmoid(write_pre)
    retain = jnp.exp(-jnp.exp(decay_log) * jax.nn.softplus(decay_pre + decay_bias))
    recalled = jnp.einsum("bhkv,bhk->bhv", old_state, keys_unit, precision=lax.Precision.HIGHEST)
    correction = values_act - retain[..., None] * recalled
    new_state = (
        retain[..., None, None] * old_state
        + (strength[..., None] * keys_unit)[..., :, None] * correction[..., None, :]
    )
    readout = jnp.einsum("bhkv,bhk->bhv", new_state, queries, precision=lax.Precision.HIGHEST)
    gated_read = readout * norm_scale(readout) * head_gain * jax.nn.silu(by_head(3))
    gated_read = gated_read.reshape(local_rows, parts, head_cols).astype(BF16)
    read_cols = exchange(gated_read.transpose(1, 0, 2)).reshape(rows, head_cols)

    partial_out = jnp.dot(read_cols, w_output, preferred_element_type=F32)
    mixer_out = exchange(partial_out.reshape(rows, parts, share).transpose(1, 0, 2)).sum(0)
    own_residual = (tokens.astype(F32) + mixer_out).astype(BF16)
    residual = gather_kv(own_residual, parts).transpose(1, 0, 2).reshape(rows, width)
    residual_wide = residual.astype(F32)
    scale_mid = norm_scale(residual_wide)
    normed_mid = (residual_wide * channel_gain).astype(BF16)
    gate_act = jnp.dot(normed_mid, w_gate, preferred_element_type=F32) * scale_mid
    upward = jnp.dot(normed_mid, w_up, preferred_element_type=F32) * scale_mid
    hidden = (jax.nn.silu(gate_act) * upward).astype(BF16)
    hidden = gather_kv(hidden, parts).transpose(1, 0, 2).reshape(rows, -1)
    down_sum = jnp.dot(hidden, w_down, preferred_element_type=F32)
    mixed = (own_residual.astype(F32) + down_sum).astype(BF16)
    return (mixed, new_state)


def solution(mesh):
    parts = mesh.shape["kv"]
    rows, states = P(("tp", "dp"), "kv"), P(("tp", "dp", "kv"), None, None, None)
    cols = P(None, "kv")
    in_specs = (rows, states, P(), cols, cols, cols, cols, P(), P(), P(), P(), P())
    in_specs += (P("kv", None), P(), cols, cols, cols)

    def step(*args):
        tokens, old_state = args[:2]
        share = tokens.shape[1]
        fits = (
            share % HEAD_DIM == 0
            and 2 * (share // HEAD_DIM) <= tokens.shape[0]
            and old_state.shape[0] == 1
            and tokens.shape[0] == parts == 8
            and args[3].shape[1] == share
            and args[14].shape[1] % 16 == 0
        )
        return (fast_body if fits else body)(*args, parts=parts)

    return jax.shard_map(
        step, mesh=mesh, in_specs=in_specs, out_specs=(rows, states), check_vma=False
    )
```

```python
import functools

import jax
import jax.numpy as jnp
from jax import lax
from jax.experimental import pallas as pl
from jax.experimental.pallas import tpu as pltpu
from jax.sharding import PartitionSpec as P

HEAD_DIM = 128
EPS = 1e-06
MIB = 1 << 20

F32, BF16 = jnp.float32, jnp.bfloat16
NEAR_FIRST = (0, 2, 3, 1, 6, 7, 4, 5)
FAR_FIRST = (0, 4, 5, 6, 7, 2, 3, 1)


def norm_scale(values):
    return lax.rsqrt(jnp.mean(values * values, axis=-1, keepdims=True) + EPS)


def unit_rows(values):
    return values * lax.rsqrt(jnp.sum(values * values, axis=-1, keepdims=True) + EPS)


def silu(values):
    return values / (1.0 + jnp.exp(-values))


def exchange(slabs):
    return lax.all_to_all(slabs, "kv", split_axis=0, concat_axis=0, tiled=True)


def swap(sent):
    parts, groups = len(sent), lax.axis_size("tp")
    got = list(sent)
    for n in range(1, parts):
        steps = [(FAR_FIRST if c else NEAR_FIRST)[n] for c in range(groups)]
        pairs = [
            (i * groups + c, (i ^ steps[c]) * groups + c)
            for i in range(parts)
            for c in range(groups)
        ]
        got[n] = lax.ppermute(sent[n], ("kv", "tp"), pairs)
    return got


def gather_kv(block, parts):
    return exchange(jnp.broadcast_to(block[None], (parts,) + block.shape))


def call(kernel, out_shape, args, *, limit=8, scratch=(), spaces=None, outs=None, span=8):
    vmem = pl.BlockSpec(memory_space=pltpu.VMEM)
    specs = [vmem] * len(args) if spaces is None else spaces
    many = isinstance(out_shape, (tuple, list))
    return pl.pallas_call(
        kernel,
        out_shape=out_shape,
        in_specs=specs,
        out_specs=outs or ([vmem] * len(out_shape) if many else vmem),
        scratch_shapes=list(scratch),
        compiler_params=pltpu.CompilerParams(vmem_limit_bytes=limit * MIB),
        cost_estimate=pl.CostEstimate(
            flops=span * 500_000_000, bytes_accessed=span * 3_000_000, transcendentals=0
        ),
    )(*args)


def eye(n):
    across = lax.broadcasted_iota(jnp.int32, (n, n), 1)
    return lax.broadcasted_iota(jnp.int32, (n, n), 0) == across


def upright(row):
    return jnp.sum(jnp.where(eye(row.shape[1]), row, 0.0), axis=1, keepdims=True)


def partners(place_ref, which_ref):
    place, far = place_ref[0], which_ref[0] > 0
    return [place ^ jnp.where(far, f, n) for f, n in zip(FAR_FIRST, NEAR_FIRST)]


def pack_kernel(place_ref, which_ref, tok_hbm, s_hbm, *refs, parts, tiles):
    outs, (buf, tok_buf, sems) = refs[:parts], refs[parts:]
    depth = tiles * HEAD_DIM
    tok_copy = pltpu.make_async_copy(tok_hbm, tok_buf, sems.at[parts])
    tok_copy.start()
    copies = []
    for x, partner in enumerate(partners(place_ref, which_ref)):
        copies.append(
            pltpu.make_async_copy(
                s_hbm.at[pl.ds(partner * tiles, tiles)], buf.at[x], sems.at[x]
            )
        )
        copies[-1].start()
    tok_copy.wait()
    tok = tok_buf[...].astype(F32)
    tok = jnp.concatenate(
        [tok[:, t * HEAD_DIM : (t + 1) * HEAD_DIM] for t in range(tiles)], axis=0
    ).astype(BF16)
    for x in range(parts):
        outs[x][depth:, :] = tok
    for x in range(parts):
        copies[x].wait()
        for t in range(tiles):
            outs[x][t * HEAD_DIM : (t + 1) * HEAD_DIM, :] = buf[x, t].astype(BF16)


def turn_kernel(after_ref, wg_hbm, wu_hbm, wg_ref, wu_ref, buf, sems):
    del after_ref
    units = wg_hbm.shape[0]
    cuts = [(a, min(a + HEAD_DIM, units)) for a in range(0, units, HEAD_DIM)]
    jobs = [(i, a, b) for i in range(2) for a, b in cuts]
    copies = [
        pltpu.make_async_copy(
            (wg_hbm, wu_hbm)[i].at[pl.ds(a, b - a)], buf.at[i, pl.ds(a, b - a)], sems.at[n]
        )
        for n, (i, a, b) in enumerate(jobs)
    ]
    for copy in copies:
        copy.start()
    for copy, (i, a, b) in zip(copies, jobs):
        copy.wait()
        (wg_ref, wu_ref)[i][:, a:b] = buf[i, a:b, :].T


def heads_kernel(
    place_ref, which_ref, gain_ref, wq, wk, wv, wg, wd_ref, ww_ref, log_ref, bias_ref,
    head_gain_ref, wo_ref, *refs, parts, tiles,
):
    slabs = refs[:parts]
    out_ref, tok_ref, retain_ref, strength_ref, kv, order = refs[parts:]
    nt = (((1,), (1,)), ((), ()))
    place = place_ref[0]
    depth = tiles * HEAD_DIM
    rows = (slabs[0].shape[0] - depth) // tiles
    sources = partners(place_ref, which_ref)
    for source, slab in zip(sources, slabs):
        order[source] = slab[depth:, :].astype(F32)
    x = jnp.concatenate(
        [order[s, t * rows : (t + 1) * rows, :] for s in range(parts) for t in range(tiles)],
        axis=-1,
    )
    tok_ref[...] = x.astype(BF16)
    width = x.shape[1]
    scale = norm_scale(x)
    normed = (x * gain_ref[...]).astype(BF16)

    decay = lax.dot_general(normed, wd_ref[...], nt, preferred_element_type=F32) * scale
    write = lax.dot_general(normed, ww_ref[...], nt, preferred_element_type=F32) * scale
    pre = decay + bias_ref[...]
    soft = jnp.maximum(pre, 0.0) + jnp.log1p(jnp.exp(-jnp.abs(pre)))
    retain_all = jnp.exp(-jnp.exp(log_ref[...]) * soft)
    strength_all = 1.0 / (1.0 + jnp.exp(-write))
    retain_ref[...] = retain_all
    strength_ref[...] = strength_all
    head = lax.broadcasted_iota(jnp.int32, retain_all.shape, 1)

    def project(w):
        acc = jnp.dot(normed, w[...], preferred_element_type=F32) * scale
        return acc.astype(BF16).astype(F32)

    query_pre, key_pre, value_pre, gate_pre = project(wq), project(wk), project(wv), project(wg)
    row = lax.broadcasted_iota(jnp.int32, (rows, HEAD_DIM), 0)
    kv[2 * tiles :] = jnp.zeros((kv.shape[0] - 2 * tiles, rows, HEAD_DIM), F32)
    gated = []
    for t in range(tiles):
        lanes = slice(t * HEAD_DIM, (t + 1) * HEAD_DIM)
        kv[t] = key_pre[:, lanes]
        kv[tiles + t] = value_pre[:, lanes]
        query = unit_rows(silu(query_pre[:, lanes])) * HEAD_DIM ** (-0.5)
        key = unit_rows(silu(key_pre[:, lanes]))
        value = silu(value_pre[:, lanes])
        own = head == place * tiles + t
        retain = jnp.sum(jnp.where(own, retain_all, 0.0), axis=1, keepdims=True)
        strength = jnp.sum(jnp.where(own, strength_all, 0.0), axis=1, keepdims=True)
        stack = []
        for vector in (key, query):
            high = vector.astype(BF16).astype(F32)
            stack += [high, vector - high]
        stack = jnp.concatenate(stack, axis=0).astype(BF16)
        found = [jnp.zeros((rows, HEAD_DIM), F32)] * 2
        for source, slab in zip(sources, slabs):
            product = jnp.dot(
                stack, slab[t * HEAD_DIM : (t + 1) * HEAD_DIM, :], preferred_element_type=F32
            )
            for i in range(2):
                both = product[2 * i * rows : (2 * i + 1) * rows] + product[
                    (2 * i + 1) * rows : (2 * i + 2) * rows
                ]
                found[i] = jnp.where(row == source, both, found[i])
        correction = value - retain * found[0]
        along = jnp.sum(key * query, axis=-1, keepdims=True)
        readout = retain * found[1] + (strength * along) * correction
        gated.append(
            readout * norm_scale(readout) * head_gain_ref[...] * silu(gate_pre[:, lanes])
        )
    gated = jnp.concatenate(gated, axis=-1).astype(BF16)
    part = jnp.dot(gated, wo_ref[...], preferred_element_type=F32).astype(BF16)
    for d in range(parts):
        out_ref[d, :, :width] = part
        out_ref[d, :, width:] = kv[:, d, :].astype(BF16)


def mixer_kernel(
    place_ref, part_ref, tok_ref, gain_ref, retain_ref, strength_ref, s_ref, wg_ref, wu_ref,
    hid_ref, res_ref, new_hbm, new, sems, *, parts, tiles,
):
    place = place_ref[0]
    width = gain_ref.shape[1]
    share = width // parts
    pre = jnp.concatenate([part_ref[j, :, width:].astype(F32) for j in range(parts)], axis=0)
    act = silu(pre)
    columns = unit_rows(act).T
    retain = jnp.broadcast_to(upright(retain_ref[pl.ds(place, 1), :]), (parts * tiles, HEAD_DIM))
    strength = jnp.broadcast_to(
        upright(strength_ref[pl.ds(place, 1), :]), (parts * tiles, HEAD_DIM)
    )
    slots = part_ref.shape[1]
    copies = []
    for j in range(parts):
        for t in range(tiles):
            h = j * tiles + t
            base = j * slots + t
            key = columns[:, base : base + 1]
            value = act[base + tiles : base + tiles + 1, :]
            old = s_ref[h]
            keep = retain[h : h + 1, :]
            recalled = jnp.sum(old * key, axis=0, keepdims=True)
            correction = (value - keep * recalled) * strength[h : h + 1, :]
            new[h] = keep * old + key * correction
        copies.append(
            pltpu.make_async_copy(
                new.at[pl.ds(j * tiles, tiles)], new_hbm.at[pl.ds(j * tiles, tiles)], sems.at[j]
            )
        )
        copies[-1].start()

    total = part_ref[0, :, :width].astype(F32)
    for s in range(1, parts):
        total = total + part_ref[s, :, :width].astype(F32)
    residual = (tok_ref[...].astype(F32) + total).astype(BF16)
    for s in range(parts):
        res_ref[s] = residual[:, s * share : (s + 1) * share]
    wide = residual.astype(F32)
    scale = norm_scale(wide)
    normed = (wide * gain_ref[...]).astype(BF16)
    gate = jnp.dot(normed, wg_ref[...], preferred_element_type=F32) * scale
    up = jnp.dot(normed, wu_ref[...], preferred_element_type=F32) * scale
    hidden = (silu(gate) * up).astype(BF16)
    for s in range(parts):
        hid_ref[s] = hidden
    for copy in copies:
        copy.wait()


def down_kernel(place_ref, hid_ref, res_ref, w_ref, out_ref, *, parts):
    units = hid_ref.shape[2]
    total = res_ref[place_ref[0]].astype(F32)
    for s in range(parts):
        total = total + jnp.dot(
            hid_ref[s], w_ref[s * units : (s + 1) * units, :], preferred_element_type=F32
        )
    out_ref[...] = total.astype(BF16)


def fast_body(
    tokens, old_state, mixer_gain, w_query, w_key, w_value, w_outgate, w_decay, w_write,
    decay_log, decay_bias, head_gain, w_output, channel_gain, w_gate, w_up, w_down, *, parts,
):
    rows, share = tokens.shape
    width = share * parts
    heads = old_state.shape[1]
    tiles = share // HEAD_DIM
    units = w_gate.shape[1]
    shape = jax.ShapeDtypeStruct
    place = lax.axis_index("kv").astype(jnp.int32).reshape(1)
    smem = pl.BlockSpec(memory_space=pltpu.SMEM)
    vmem = pl.BlockSpec(memory_space=pltpu.VMEM)
    hbm = pl.BlockSpec(memory_space=pltpu.HBM)
    states = (heads, HEAD_DIM, HEAD_DIM)
    state = old_state[0]

    which = lax.axis_index("tp").astype(jnp.int32).reshape(1)
    tokens, place, which = lax.optimization_barrier((tokens, place, which))
    slab = shape((tiles * (HEAD_DIM + rows), HEAD_DIM), BF16)
    sent = call(
        functools.partial(pack_kernel, parts=parts, tiles=tiles),
        [slab] * parts,
        (place, which, pltpu.with_memory_space_constraint(tokens, pltpu.HBM),
         pltpu.with_memory_space_constraint(state, pltpu.HBM)),
        scratch=[
            pltpu.VMEM((parts, tiles) + states[1:], F32),
            pltpu.VMEM((rows, share), BF16),
            pltpu.SemaphoreType.DMA((parts + 1,)),
        ],
        spaces=[smem, smem, hbm, hbm],
        span=1,
    )
    slabs = swap(sent)
    turned = shape((width, units), BF16)
    wide_gate, wide_up = call(
        turn_kernel,
        (turned, turned),
        (sent[0], pltpu.with_memory_space_constraint(w_gate.T, pltpu.HBM),
         pltpu.with_memory_space_constraint(w_up.T, pltpu.HBM)),
        scratch=[
            pltpu.VMEM((2, units, width), BF16),
            pltpu.SemaphoreType.DMA((2 * pl.cdiv(units, HEAD_DIM),)),
        ],
        spaces=[vmem, hbm, hbm],
        limit=16,
        span=40,
    )
    slabs, wide_gate, wide_up = lax.optimization_barrier((slabs, wide_gate, wide_up))
    part, wide, retain, strength = call(
        functools.partial(heads_kernel, parts=parts, tiles=tiles),
        (
            shape((parts, rows, width + HEAD_DIM), BF16),
            shape((rows, width), BF16),
            shape((rows, heads), F32),
            shape((rows, heads), F32),
        ),
        (
            place, which, mixer_gain.reshape(1, width), w_query, w_key, w_value, w_outgate,
            w_decay.T, w_write.T, decay_log.reshape(1, heads), decay_bias.reshape(1, heads),
            head_gain.reshape(1, HEAD_DIM), w_output, *slabs,
        ),
        scratch=[
            pltpu.VMEM((rows, rows, HEAD_DIM), F32),
            pltpu.VMEM((parts, tiles * rows, HEAD_DIM), F32),
        ],
        spaces=[smem] * 2 + [vmem] * (11 + parts),
    )
    part = exchange(part)
    hidden, residual, new_state = call(
        functools.partial(mixer_kernel, parts=parts, tiles=tiles),
        (
            shape((parts, rows, units), BF16),
            shape((parts, rows, share), BF16),
            shape(states, F32),
        ),
        (
            place, part, wide, channel_gain.reshape(1, width), retain, strength, state,
            wide_gate, wide_up,
        ),
        scratch=[pltpu.VMEM(states, F32), pltpu.SemaphoreType.DMA((parts,))],
        spaces=[smem] + [vmem] * 8,
        outs=[vmem, vmem, hbm],
    )
    hidden = exchange(hidden)
    mixed = call(
        functools.partial(down_kernel, parts=parts),
        shape((rows, share), BF16),
        (place, hidden, residual, w_down),
        spaces=[smem] + [vmem] * 3,
    )
    return mixed, new_state[None]


def body(
    tokens, old_state, mixer_gain, w_query, w_key, w_value, w_outgate, w_decay, w_write,
    decay_log, decay_bias, head_gain, w_output, channel_gain, w_gate, w_up, w_down, *, parts,
):
    rows, share = tokens.shape
    width = share * parts
    local_rows, heads = old_state.shape[:2]
    head_cols = w_query.shape[1]
    place = lax.axis_index("kv")

    tok_wide = gather_kv(tokens, parts).transpose(1, 0, 2).reshape(rows, width).astype(F32)
    scale_in = norm_scale(tok_wide)
    normed = (tok_wide * mixer_gain).astype(BF16)

    def project(weight):
        return (jnp.dot(normed, weight, preferred_element_type=F32) * scale_in).astype(BF16)

    packed = jnp.stack([project(w) for w in (w_query, w_key, w_value, w_outgate)], axis=1)
    packed = exchange(packed.reshape(parts, local_rows, 4, head_cols))

    own_normed = lax.dynamic_slice_in_dim(normed, place * local_rows, local_rows, 0)
    own_scale = lax.dynamic_slice_in_dim(scale_in, place * local_rows, local_rows, 0)
    decay_pre = jnp.dot(own_normed, w_decay, preferred_element_type=F32) * own_scale
    write_pre = jnp.dot(own_normed, w_write, preferred_element_type=F32) * own_scale

    def by_head(index):
        chosen = packed[:, :, index].transpose(1, 0, 2)
        return chosen.reshape(local_rows, heads, HEAD_DIM).astype(F32)

    queries = unit_rows(jax.nn.silu(by_head(0))) * HEAD_DIM ** (-0.5)
    keys_unit = unit_rows(jax.nn.silu(by_head(1)))
    values_act = jax.nn.silu(by_head(2))
    strength = jax.nn.sigmoid(write_pre)
    retain = jnp.exp(-jnp.exp(decay_log) * jax.nn.softplus(decay_pre + decay_bias))
    recalled = jnp.einsum("bhkv,bhk->bhv", old_state, keys_unit, precision=lax.Precision.HIGHEST)
    correction = values_act - retain[..., None] * recalled
    new_state = (
        retain[..., None, None] * old_state
        + (strength[..., None] * keys_unit)[..., :, None] * correction[..., None, :]
    )
    readout = jnp.einsum("bhkv,bhk->bhv", new_state, queries, precision=lax.Precision.HIGHEST)
    gated_read = readout * norm_scale(readout) * head_gain * jax.nn.silu(by_head(3))
    gated_read = gated_read.reshape(local_rows, parts, head_cols).astype(BF16)
    read_cols = exchange(gated_read.transpose(1, 0, 2)).reshape(rows, head_cols)

    partial_out = jnp.dot(read_cols, w_output, preferred_element_type=F32)
    mixer_out = exchange(partial_out.reshape(rows, parts, share).transpose(1, 0, 2)).sum(0)
    own_residual = (tokens.astype(F32) + mixer_out).astype(BF16)
    residual = gather_kv(own_residual, parts).transpose(1, 0, 2).reshape(rows, width)
    residual_wide = residual.astype(F32)
    scale_mid = norm_scale(residual_wide)
    normed_mid = (residual_wide * channel_gain).astype(BF16)
    gate_act = jnp.dot(normed_mid, w_gate, preferred_element_type=F32) * scale_mid
    upward = jnp.dot(normed_mid, w_up, preferred_element_type=F32) * scale_mid
    hidden = (jax.nn.silu(gate_act) * upward).astype(BF16)
    hidden = gather_kv(hidden, parts).transpose(1, 0, 2).reshape(rows, -1)
    down_sum = jnp.dot(hidden, w_down, preferred_element_type=F32)
    mixed = (own_residual.astype(F32) + down_sum).astype(BF16)
    return (mixed, new_state)


def solution(mesh):
    parts = mesh.shape["kv"]
    rows, states = P(("tp", "dp"), "kv"), P(("tp", "dp", "kv"), None, None, None)
    cols = P(None, "kv")
    in_specs = (rows, states, P(), cols, cols, cols, cols, P(), P(), P(), P(), P())
    in_specs += (P("kv", None), P(), cols, cols, cols)

    def step(*args):
        tokens, old_state = args[:2]
        share = tokens.shape[1]
        fits = (
            share % HEAD_DIM == 0
            and 2 * (share // HEAD_DIM) <= tokens.shape[0]
            and old_state.shape[0] == 1
            and tokens.shape[0] == parts == 8
            and args[3].shape[1] == share
            and args[14].shape[1] % 16 == 0
        )
        return (fast_body if fits else body)(*args, parts=parts)

    return jax.shard_map(
        step, mesh=mesh, in_specs=in_specs, out_specs=(rows, states), check_vma=False
    )
```

```python
import functools

import jax
import jax.numpy as jnp
from jax import lax
from jax.experimental import pallas as pl
from jax.experimental.pallas import tpu as pltpu
from jax.sharding import PartitionSpec as P

HEAD_DIM = 128
EPS = 1e-06
MIB = 1 << 20

F32, BF16 = jnp.float32, jnp.bfloat16
NEAR_FIRST = (0, 2, 3, 1, 4, 5, 6, 7)
FAR_FIRST = (0, 4, 5, 6, 7, 2, 3, 1)


def norm_scale(values):
    return lax.rsqrt(jnp.mean(values * values, axis=-1, keepdims=True) + EPS)


def unit_rows(values):
    return values * lax.rsqrt(jnp.sum(values * values, axis=-1, keepdims=True) + EPS)


def silu(values):
    return values / (1.0 + jnp.exp(-values))


def exchange(slabs):
    return lax.all_to_all(slabs, "kv", split_axis=0, concat_axis=0, tiled=True)


def swap(sent):
    parts, groups = len(sent), lax.axis_size("tp")
    got = list(sent)
    for n in range(1, parts):
        steps = [(FAR_FIRST if c else NEAR_FIRST)[n] for c in range(groups)]
        pairs = [
            (i * groups + c, (i ^ steps[c]) * groups + c)
            for i in range(parts)
            for c in range(groups)
        ]
        got[n] = lax.ppermute(sent[n], ("kv", "tp"), pairs)
    return got


def gather_kv(block, parts):
    return exchange(jnp.broadcast_to(block[None], (parts,) + block.shape))


def call(kernel, out_shape, args, *, limit=8, scratch=(), spaces=None, outs=None, span=8):
    vmem = pl.BlockSpec(memory_space=pltpu.VMEM)
    specs = [vmem] * len(args) if spaces is None else spaces
    many = isinstance(out_shape, (tuple, list))
    return pl.pallas_call(
        kernel,
        out_shape=out_shape,
        in_specs=specs,
        out_specs=outs or ([vmem] * len(out_shape) if many else vmem),
        scratch_shapes=list(scratch),
        compiler_params=pltpu.CompilerParams(vmem_limit_bytes=limit * MIB),
        cost_estimate=pl.CostEstimate(
            flops=span * 500_000_000, bytes_accessed=span * 3_000_000, transcendentals=0
        ),
    )(*args)


def eye(n):
    across = lax.broadcasted_iota(jnp.int32, (n, n), 1)
    return lax.broadcasted_iota(jnp.int32, (n, n), 0) == across


def upright(row):
    return jnp.sum(jnp.where(eye(row.shape[1]), row, 0.0), axis=1, keepdims=True)


def partners(place_ref, which_ref):
    place, far = place_ref[0], which_ref[0] > 0
    return [place ^ jnp.where(far, f, n) for f, n in zip(FAR_FIRST, NEAR_FIRST)]


def pack_kernel(place_ref, which_ref, tok_hbm, s_hbm, *refs, parts, tiles):
    outs, (buf, tok_buf, sems) = refs[:parts], refs[parts:]
    depth = tiles * HEAD_DIM
    tok_copy = pltpu.make_async_copy(tok_hbm, tok_buf, sems.at[parts])
    tok_copy.start()
    copies = []
    for x, partner in enumerate(partners(place_ref, which_ref)):
        copies.append(
            pltpu.make_async_copy(
                s_hbm.at[pl.ds(partner * tiles, tiles)], buf.at[x], sems.at[x]
            )
        )
        copies[-1].start()
    tok_copy.wait()
    tok = tok_buf[...].astype(F32)
    tok = jnp.concatenate(
        [tok[:, t * HEAD_DIM : (t + 1) * HEAD_DIM] for t in range(tiles)], axis=0
    ).astype(BF16)
    for x in range(parts):
        outs[x][depth:, :] = tok
    for x in range(parts):
        copies[x].wait()
        for t in range(tiles):
            outs[x][t * HEAD_DIM : (t + 1) * HEAD_DIM, :] = buf[x, t].astype(BF16)


def turn_kernel(after_ref, wg_hbm, wu_hbm, wg_ref, wu_ref, buf, sems):
    del after_ref
    units = wg_hbm.shape[0]
    cuts = [(a, min(a + HEAD_DIM, units)) for a in range(0, units, HEAD_DIM)]
    jobs = [(i, a, b) for i in range(2) for a, b in cuts]
    copies = [
        pltpu.make_async_copy(
            (wg_hbm, wu_hbm)[i].at[pl.ds(a, b - a)], buf.at[i, pl.ds(a, b - a)], sems.at[n]
        )
        for n, (i, a, b) in enumerate(jobs)
    ]
    for copy in copies:
        copy.start()
    for copy, (i, a, b) in zip(copies, jobs):
        copy.wait()
        (wg_ref, wu_ref)[i][:, a:b] = buf[i, a:b, :].T


def heads_kernel(
    place_ref, which_ref, gain_ref, wq, wk, wv, wg, wd_ref, ww_ref, log_ref, bias_ref,
    head_gain_ref, wo_ref, *refs, parts, tiles,
):
    slabs = refs[:parts]
    out_ref, tok_ref, retain_ref, strength_ref, kv, order = refs[parts:]
    nt = (((1,), (1,)), ((), ()))
    place = place_ref[0]
    depth = tiles * HEAD_DIM
    rows = (slabs[0].shape[0] - depth) // tiles
    sources = partners(place_ref, which_ref)
    for source, slab in zip(sources, slabs):
        order[source] = slab[depth:, :].astype(F32)
    x = jnp.concatenate(
        [order[s, t * rows : (t + 1) * rows, :] for s in range(parts) for t in range(tiles)],
        axis=-1,
    )
    tok_ref[...] = x.astype(BF16)
    width = x.shape[1]
    scale = norm_scale(x)
    normed = (x * gain_ref[...]).astype(BF16)

    decay = lax.dot_general(normed, wd_ref[...], nt, preferred_element_type=F32) * scale
    write = lax.dot_general(normed, ww_ref[...], nt, preferred_element_type=F32) * scale
    pre = decay + bias_ref[...]
    soft = jnp.maximum(pre, 0.0) + jnp.log1p(jnp.exp(-jnp.abs(pre)))
    retain_all = jnp.exp(-jnp.exp(log_ref[...]) * soft)
    strength_all = 1.0 / (1.0 + jnp.exp(-write))
    retain_ref[...] = retain_all
    strength_ref[...] = strength_all
    head = lax.broadcasted_iota(jnp.int32, retain_all.shape, 1)

    def project(w):
        acc = jnp.dot(normed, w[...], preferred_element_type=F32) * scale
        return acc.astype(BF16).astype(F32)

    query_pre, key_pre, value_pre, gate_pre = project(wq), project(wk), project(wv), project(wg)
    row = lax.broadcasted_iota(jnp.int32, (rows, HEAD_DIM), 0)
    kv[2 * tiles :] = jnp.zeros((kv.shape[0] - 2 * tiles, rows, HEAD_DIM), F32)
    gated = []
    for t in range(tiles):
        lanes = slice(t * HEAD_DIM, (t + 1) * HEAD_DIM)
        kv[t] = key_pre[:, lanes]
        kv[tiles + t] = value_pre[:, lanes]
        query = unit_rows(silu(query_pre[:, lanes])) * HEAD_DIM ** (-0.5)
        key = unit_rows(silu(key_pre[:, lanes]))
        value = silu(value_pre[:, lanes])
        own = head == place * tiles + t
        retain = jnp.sum(jnp.where(own, retain_all, 0.0), axis=1, keepdims=True)
        strength = jnp.sum(jnp.where(own, strength_all, 0.0), axis=1, keepdims=True)
        stack = []
        for vector in (key, query):
            high = vector.astype(BF16).astype(F32)
            stack += [high, vector - high]
        stack = jnp.concatenate(stack, axis=0).astype(BF16)
        found = [jnp.zeros((rows, HEAD_DIM), F32)] * 2
        for source, slab in zip(sources, slabs):
            product = jnp.dot(
                stack, slab[t * HEAD_DIM : (t + 1) * HEAD_DIM, :], preferred_element_type=F32
            )
            for i in range(2):
                both = product[2 * i * rows : (2 * i + 1) * rows] + product[
                    (2 * i + 1) * rows : (2 * i + 2) * rows
                ]
                found[i] = jnp.where(row == source, both, found[i])
        correction = value - retain * found[0]
        along = jnp.sum(key * query, axis=-1, keepdims=True)
        readout = retain * found[1] + (strength * along) * correction
        gated.append(
            readout * norm_scale(readout) * head_gain_ref[...] * silu(gate_pre[:, lanes])
        )
    gated = jnp.concatenate(gated, axis=-1).astype(BF16)
    part = jnp.dot(gated, wo_ref[...], preferred_element_type=F32).astype(BF16)
    for d in range(parts):
        out_ref[d, :, :width] = part
        out_ref[d, :, width:] = kv[:, d, :].astype(BF16)


def mixer_kernel(
    place_ref, part_ref, tok_ref, gain_ref, retain_ref, strength_ref, s_ref, wg_ref, wu_ref,
    hid_ref, res_ref, new_hbm, new, sems, *, parts, tiles,
):
    place = place_ref[0]
    width = gain_ref.shape[1]
    share = width // parts
    pre = jnp.concatenate([part_ref[j, :, width:].astype(F32) for j in range(parts)], axis=0)
    act = silu(pre)
    columns = unit_rows(act).T
    retain = jnp.broadcast_to(upright(retain_ref[pl.ds(place, 1), :]), (parts * tiles, HEAD_DIM))
    strength = jnp.broadcast_to(
        upright(strength_ref[pl.ds(place, 1), :]), (parts * tiles, HEAD_DIM)
    )
    slots = part_ref.shape[1]
    copies = []
    for j in range(parts):
        for t in range(tiles):
            h = j * tiles + t
            base = j * slots + t
            key = columns[:, base : base + 1]
            value = act[base + tiles : base + tiles + 1, :]
            old = s_ref[h]
            keep = retain[h : h + 1, :]
            recalled = jnp.sum(old * key, axis=0, keepdims=True)
            correction = (value - keep * recalled) * strength[h : h + 1, :]
            new[h] = keep * old + key * correction
        copies.append(
            pltpu.make_async_copy(
                new.at[pl.ds(j * tiles, tiles)], new_hbm.at[pl.ds(j * tiles, tiles)], sems.at[j]
            )
        )
        copies[-1].start()

    total = part_ref[0, :, :width].astype(F32)
    for s in range(1, parts):
        total = total + part_ref[s, :, :width].astype(F32)
    residual = (tok_ref[...].astype(F32) + total).astype(BF16)
    for s in range(parts):
        res_ref[s] = residual[:, s * share : (s + 1) * share]
    wide = residual.astype(F32)
    scale = norm_scale(wide)
    normed = (wide * gain_ref[...]).astype(BF16)
    gate = jnp.dot(normed, wg_ref[...], preferred_element_type=F32) * scale
    up = jnp.dot(normed, wu_ref[...], preferred_element_type=F32) * scale
    hidden = (silu(gate) * up).astype(BF16)
    for s in range(parts):
        hid_ref[s] = hidden
    for copy in copies:
        copy.wait()


def down_kernel(place_ref, hid_ref, res_ref, w_ref, out_ref, *, parts):
    units = hid_ref.shape[2]
    total = res_ref[place_ref[0]].astype(F32)
    for s in range(parts):
        total = total + jnp.dot(
            hid_ref[s], w_ref[s * units : (s + 1) * units, :], preferred_element_type=F32
        )
    out_ref[...] = total.astype(BF16)


def fast_body(
    tokens, old_state, mixer_gain, w_query, w_key, w_value, w_outgate, w_decay, w_write,
    decay_log, decay_bias, head_gain, w_output, channel_gain, w_gate, w_up, w_down, *, parts,
):
    rows, share = tokens.shape
    width = share * parts
    heads = old_state.shape[1]
    tiles = share // HEAD_DIM
    units = w_gate.shape[1]
    shape = jax.ShapeDtypeStruct
    place = lax.axis_index("kv").astype(jnp.int32).reshape(1)
    smem = pl.BlockSpec(memory_space=pltpu.SMEM)
    vmem = pl.BlockSpec(memory_space=pltpu.VMEM)
    hbm = pl.BlockSpec(memory_space=pltpu.HBM)
    states = (heads, HEAD_DIM, HEAD_DIM)
    state = old_state[0]

    which = lax.axis_index("tp").astype(jnp.int32).reshape(1)
    tokens, place, which = lax.optimization_barrier((tokens, place, which))
    slab = shape((tiles * (HEAD_DIM + rows), HEAD_DIM), BF16)
    sent = call(
        functools.partial(pack_kernel, parts=parts, tiles=tiles),
        [slab] * parts,
        (place, which, pltpu.with_memory_space_constraint(tokens, pltpu.HBM),
         pltpu.with_memory_space_constraint(state, pltpu.HBM)),
        scratch=[
            pltpu.VMEM((parts, tiles) + states[1:], F32),
            pltpu.VMEM((rows, share), BF16),
            pltpu.SemaphoreType.DMA((parts + 1,)),
        ],
        spaces=[smem, smem, hbm, hbm],
        span=1,
    )
    slabs = swap(sent)
    turned = shape((width, units), BF16)
    wide_gate, wide_up = call(
        turn_kernel,
        (turned, turned),
        (sent[0], pltpu.with_memory_space_constraint(w_gate.T, pltpu.HBM),
         pltpu.with_memory_space_constraint(w_up.T, pltpu.HBM)),
        scratch=[
            pltpu.VMEM((2, units, width), BF16),
            pltpu.SemaphoreType.DMA((2 * pl.cdiv(units, HEAD_DIM),)),
        ],
        spaces=[vmem, hbm, hbm],
        limit=16,
        span=40,
    )
    slabs, wide_gate, wide_up = lax.optimization_barrier((slabs, wide_gate, wide_up))
    part, wide, retain, strength = call(
        functools.partial(heads_kernel, parts=parts, tiles=tiles),
        (
            shape((parts, rows, width + HEAD_DIM), BF16),
            shape((rows, width), BF16),
            shape((rows, heads), F32),
            shape((rows, heads), F32),
        ),
        (
            place, which, mixer_gain.reshape(1, width), w_query, w_key, w_value, w_outgate,
            w_decay.T, w_write.T, decay_log.reshape(1, heads), decay_bias.reshape(1, heads),
            head_gain.reshape(1, HEAD_DIM), w_output, *slabs,
        ),
        scratch=[
            pltpu.VMEM((rows, rows, HEAD_DIM), F32),
            pltpu.VMEM((parts, tiles * rows, HEAD_DIM), F32),
        ],
        spaces=[smem] * 2 + [vmem] * (11 + parts),
    )
    part = exchange(part)
    hidden, residual, new_state = call(
        functools.partial(mixer_kernel, parts=parts, tiles=tiles),
        (
            shape((parts, rows, units), BF16),
            shape((parts, rows, share), BF16),
            shape(states, F32),
        ),
        (
            place, part, wide, channel_gain.reshape(1, width), retain, strength, state,
            wide_gate, wide_up,
        ),
        scratch=[pltpu.VMEM(states, F32), pltpu.SemaphoreType.DMA((parts,))],
        spaces=[smem] + [vmem] * 8,
        outs=[vmem, vmem, hbm],
    )
    hidden = exchange(hidden)
    mixed = call(
        functools.partial(down_kernel, parts=parts),
        shape((rows, share), BF16),
        (place, hidden, residual, w_down),
        spaces=[smem] + [vmem] * 3,
    )
    return mixed, new_state[None]


def body(
    tokens, old_state, mixer_gain, w_query, w_key, w_value, w_outgate, w_decay, w_write,
    decay_log, decay_bias, head_gain, w_output, channel_gain, w_gate, w_up, w_down, *, parts,
):
    rows, share = tokens.shape
    width = share * parts
    local_rows, heads = old_state.shape[:2]
    head_cols = w_query.shape[1]
    place = lax.axis_index("kv")

    tok_wide = gather_kv(tokens, parts).transpose(1, 0, 2).reshape(rows, width).astype(F32)
    scale_in = norm_scale(tok_wide)
    normed = (tok_wide * mixer_gain).astype(BF16)

    def project(weight):
        return (jnp.dot(normed, weight, preferred_element_type=F32) * scale_in).astype(BF16)

    packed = jnp.stack([project(w) for w in (w_query, w_key, w_value, w_outgate)], axis=1)
    packed = exchange(packed.reshape(parts, local_rows, 4, head_cols))

    own_normed = lax.dynamic_slice_in_dim(normed, place * local_rows, local_rows, 0)
    own_scale = lax.dynamic_slice_in_dim(scale_in, place * local_rows, local_rows, 0)
    decay_pre = jnp.dot(own_normed, w_decay, preferred_element_type=F32) * own_scale
    write_pre = jnp.dot(own_normed, w_write, preferred_element_type=F32) * own_scale

    def by_head(index):
        chosen = packed[:, :, index].transpose(1, 0, 2)
        return chosen.reshape(local_rows, heads, HEAD_DIM).astype(F32)

    queries = unit_rows(jax.nn.silu(by_head(0))) * HEAD_DIM ** (-0.5)
    keys_unit = unit_rows(jax.nn.silu(by_head(1)))
    values_act = jax.nn.silu(by_head(2))
    strength = jax.nn.sigmoid(write_pre)
    retain = jnp.exp(-jnp.exp(decay_log) * jax.nn.softplus(decay_pre + decay_bias))
    recalled = jnp.einsum("bhkv,bhk->bhv", old_state, keys_unit, precision=lax.Precision.HIGHEST)
    correction = values_act - retain[..., None] * recalled
    new_state = (
        retain[..., None, None] * old_state
        + (strength[..., None] * keys_unit)[..., :, None] * correction[..., None, :]
    )
    readout = jnp.einsum("bhkv,bhk->bhv", new_state, queries, precision=lax.Precision.HIGHEST)
    gated_read = readout * norm_scale(readout) * head_gain * jax.nn.silu(by_head(3))
    gated_read = gated_read.reshape(local_rows, parts, head_cols).astype(BF16)
    read_cols = exchange(gated_read.transpose(1, 0, 2)).reshape(rows, head_cols)

    partial_out = jnp.dot(read_cols, w_output, preferred_element_type=F32)
    mixer_out = exchange(partial_out.reshape(rows, parts, share).transpose(1, 0, 2)).sum(0)
    own_residual = (tokens.astype(F32) + mixer_out).astype(BF16)
    residual = gather_kv(own_residual, parts).transpose(1, 0, 2).reshape(rows, width)
    residual_wide = residual.astype(F32)
    scale_mid = norm_scale(residual_wide)
    normed_mid = (residual_wide * channel_gain).astype(BF16)
    gate_act = jnp.dot(normed_mid, w_gate, preferred_element_type=F32) * scale_mid
    upward = jnp.dot(normed_mid, w_up, preferred_element_type=F32) * scale_mid
    hidden = (jax.nn.silu(gate_act) * upward).astype(BF16)
    hidden = gather_kv(hidden, parts).transpose(1, 0, 2).reshape(rows, -1)
    down_sum = jnp.dot(hidden, w_down, preferred_element_type=F32)
    mixed = (own_residual.astype(F32) + down_sum).astype(BF16)
    return (mixed, new_state)


def solution(mesh):
    parts = mesh.shape["kv"]
    rows, states = P(("tp", "dp"), "kv"), P(("tp", "dp", "kv"), None, None, None)
    cols = P(None, "kv")
    in_specs = (rows, states, P(), cols, cols, cols, cols, P(), P(), P(), P(), P())
    in_specs += (P("kv", None), P(), cols, cols, cols)

    def step(*args):
        tokens, old_state = args[:2]
        share = tokens.shape[1]
        fits = (
            share % HEAD_DIM == 0
            and 2 * (share // HEAD_DIM) <= tokens.shape[0]
            and old_state.shape[0] == 1
            and tokens.shape[0] == parts == 8
            and args[3].shape[1] == share
            and args[14].shape[1] % 16 == 0
        )
        return (fast_body if fits else body)(*args, parts=parts)

    return jax.shard_map(
        step, mesh=mesh, in_specs=in_specs, out_specs=(rows, states), check_vma=False
    )
```

```python
import functools

import jax
import jax.numpy as jnp
from jax import lax
from jax.experimental import pallas as pl
from jax.experimental.pallas import tpu as pltpu
from jax.sharding import PartitionSpec as P

HEAD_DIM = 128
EPS = 1e-06
MIB = 1 << 20

F32, BF16 = jnp.float32, jnp.bfloat16
NEAR_FIRST = (0, 2, 3, 1, 4, 5, 6, 7)
FAR_FIRST = (0, 4, 5, 6, 7, 2, 3, 1)


def norm_scale(values):
    return lax.rsqrt(jnp.mean(values * values, axis=-1, keepdims=True) + EPS)


def unit_rows(values):
    return values * lax.rsqrt(jnp.sum(values * values, axis=-1, keepdims=True) + EPS)


def silu(values):
    return values / (1.0 + jnp.exp(-values))


def exchange(slabs):
    return lax.all_to_all(slabs, "kv", split_axis=0, concat_axis=0, tiled=True)


def swap(sent):
    parts, groups = len(sent), lax.axis_size("tp")
    got = list(sent)
    for n in range(1, parts):
        steps = [(FAR_FIRST if c else NEAR_FIRST)[n] for c in range(groups)]
        pairs = [
            (i * groups + c, (i ^ steps[c]) * groups + c)
            for i in range(parts)
            for c in range(groups)
        ]
        got[n] = lax.ppermute(sent[n], ("kv", "tp"), pairs)
    return got


def gather_kv(block, parts):
    return exchange(jnp.broadcast_to(block[None], (parts,) + block.shape))


def call(kernel, out_shape, args, *, limit=8, scratch=(), spaces=None, outs=None, span=8):
    vmem = pl.BlockSpec(memory_space=pltpu.VMEM)
    specs = [vmem] * len(args) if spaces is None else spaces
    many = isinstance(out_shape, (tuple, list))
    return pl.pallas_call(
        kernel,
        out_shape=out_shape,
        in_specs=specs,
        out_specs=outs or ([vmem] * len(out_shape) if many else vmem),
        scratch_shapes=list(scratch),
        compiler_params=pltpu.CompilerParams(vmem_limit_bytes=limit * MIB),
        cost_estimate=pl.CostEstimate(
            flops=span * 500_000_000, bytes_accessed=span * 3_000_000, transcendentals=0
        ),
    )(*args)


def eye(n):
    across = lax.broadcasted_iota(jnp.int32, (n, n), 1)
    return lax.broadcasted_iota(jnp.int32, (n, n), 0) == across


def upright(row):
    return jnp.sum(jnp.where(eye(row.shape[1]), row, 0.0), axis=1, keepdims=True)


def partners(place_ref, which_ref):
    place, far = place_ref[0], which_ref[0] > 0
    return [place ^ jnp.where(far, f, n) for f, n in zip(FAR_FIRST, NEAR_FIRST)]


def pack_kernel(place_ref, which_ref, tok_hbm, s_hbm, *refs, parts, tiles):
    outs, (buf, tok_buf, sems) = refs[:parts], refs[parts:]
    depth = tiles * HEAD_DIM
    tok_copy = pltpu.make_async_copy(tok_hbm, tok_buf, sems.at[parts])
    tok_copy.start()
    copies = []
    for x, partner in enumerate(partners(place_ref, which_ref)):
        copies.append(
            pltpu.make_async_copy(
                s_hbm.at[pl.ds(partner * tiles, tiles)], buf.at[x], sems.at[x]
            )
        )
        copies[-1].start()
    tok_copy.wait()
    tok = tok_buf[...].astype(F32)
    tok = jnp.concatenate(
        [tok[:, t * HEAD_DIM : (t + 1) * HEAD_DIM] for t in range(tiles)], axis=0
    ).astype(BF16)
    for x in range(parts):
        outs[x][depth:, :] = tok
    for x in range(parts):
        copies[x].wait()
        for t in range(tiles):
            outs[x][t * HEAD_DIM : (t + 1) * HEAD_DIM, :] = buf[x, t].astype(BF16)


def turn_kernel(after_ref, wg_hbm, wu_hbm, wg_ref, wu_ref, buf, sems):
    del after_ref
    units = wg_hbm.shape[0]
    cuts = [(a, min(a + HEAD_DIM, units)) for a in range(0, units, HEAD_DIM)]
    jobs = [(i, a, b) for i in range(2) for a, b in cuts]
    copies = [
        pltpu.make_async_copy(
            (wg_hbm, wu_hbm)[i].at[pl.ds(a, b - a)], buf.at[i, pl.ds(a, b - a)], sems.at[n]
        )
        for n, (i, a, b) in enumerate(jobs)
    ]
    for copy in copies:
        copy.start()
    for copy, (i, a, b) in zip(copies, jobs):
        copy.wait()
        (wg_ref, wu_ref)[i][:, a:b] = buf[i, a:b, :].T


def heads_kernel(
    place_ref, which_ref, gain_ref, wq, wk, wv, wg, wd_ref, ww_ref, log_ref, bias_ref,
    head_gain_ref, wo_ref, *refs, parts, tiles,
):
    slabs = refs[:parts]
    out_ref, tok_ref, retain_ref, strength_ref, kv, order = refs[parts:]
    nt = (((1,), (1,)), ((), ()))
    place = place_ref[0]
    depth = tiles * HEAD_DIM
    rows = (slabs[0].shape[0] - depth) // tiles
    sources = partners(place_ref, which_ref)
    for source, slab in zip(sources, slabs):
        order[source] = slab[depth:, :].astype(F32)
    x = jnp.concatenate(
        [order[s, t * rows : (t + 1) * rows, :] for s in range(parts) for t in range(tiles)],
        axis=-1,
    )
    tok_ref[...] = x.astype(BF16)
    width = x.shape[1]
    scale = norm_scale(x)
    normed = (x * gain_ref[...]).astype(BF16)

    decay = lax.dot_general(normed, wd_ref[...], nt, preferred_element_type=F32) * scale
    write = lax.dot_general(normed, ww_ref[...], nt, preferred_element_type=F32) * scale
    pre = decay + bias_ref[...]
    soft = jnp.maximum(pre, 0.0) + jnp.log1p(jnp.exp(-jnp.abs(pre)))
    retain_all = jnp.exp(-jnp.exp(log_ref[...]) * soft)
    strength_all = 1.0 / (1.0 + jnp.exp(-write))
    retain_ref[...] = retain_all
    strength_ref[...] = strength_all
    head = lax.broadcasted_iota(jnp.int32, retain_all.shape, 1)

    def project(w):
        acc = jnp.dot(normed, w[...], preferred_element_type=F32) * scale
        return acc.astype(BF16).astype(F32)

    query_pre, key_pre, value_pre, gate_pre = project(wq), project(wk), project(wv), project(wg)
    row = lax.broadcasted_iota(jnp.int32, (rows, HEAD_DIM), 0)
    kv[2 * tiles :] = jnp.zeros((kv.shape[0] - 2 * tiles, rows, HEAD_DIM), F32)
    gated = []
    for t in range(tiles):
        lanes = slice(t * HEAD_DIM, (t + 1) * HEAD_DIM)
        kv[t] = key_pre[:, lanes]
        kv[tiles + t] = value_pre[:, lanes]
        query = unit_rows(silu(query_pre[:, lanes])) * HEAD_DIM ** (-0.5)
        key = unit_rows(silu(key_pre[:, lanes]))
        value = silu(value_pre[:, lanes])
        own = head == place * tiles + t
        retain = jnp.sum(jnp.where(own, retain_all, 0.0), axis=1, keepdims=True)
        strength = jnp.sum(jnp.where(own, strength_all, 0.0), axis=1, keepdims=True)
        stack = []
        for vector in (key, query):
            high = vector.astype(BF16).astype(F32)
            stack += [high, vector - high]
        stack = jnp.concatenate(stack, axis=0).astype(BF16)
        found = [jnp.zeros((rows, HEAD_DIM), F32)] * 2
        for source, slab in zip(sources, slabs):
            product = jnp.dot(
                stack, slab[t * HEAD_DIM : (t + 1) * HEAD_DIM, :], preferred_element_type=F32
            )
            for i in range(2):
                both = product[2 * i * rows : (2 * i + 1) * rows] + product[
                    (2 * i + 1) * rows : (2 * i + 2) * rows
                ]
                found[i] = jnp.where(row == source, both, found[i])
        correction = value - retain * found[0]
        along = jnp.sum(key * query, axis=-1, keepdims=True)
        readout = retain * found[1] + (strength * along) * correction
        gated.append(
            readout * norm_scale(readout) * head_gain_ref[...] * silu(gate_pre[:, lanes])
        )
    gated = jnp.concatenate(gated, axis=-1).astype(BF16)
    part = jnp.dot(gated, wo_ref[...], preferred_element_type=F32).astype(BF16)
    for d in range(parts):
        out_ref[d, :, :width] = part
        out_ref[d, :, width:] = kv[:, d, :].astype(BF16)


def mixer_kernel(
    place_ref, part_ref, tok_ref, gain_ref, retain_ref, strength_ref, s_ref, wg_ref, wu_ref,
    hid_ref, res_ref, new_hbm, new, sems, *, parts, tiles,
):
    place = place_ref[0]
    width = gain_ref.shape[1]
    share = width // parts
    total = part_ref[0, :, :width].astype(F32)
    for s in range(1, parts):
        total = total + part_ref[s, :, :width].astype(F32)
    residual = (tok_ref[...].astype(F32) + total).astype(BF16)
    for s in range(parts):
        res_ref[s] = residual[:, s * share : (s + 1) * share]
    wide = residual.astype(F32)
    scale = norm_scale(wide)
    normed = (wide * gain_ref[...]).astype(BF16)
    gate = jnp.dot(normed, wg_ref[...], preferred_element_type=F32) * scale
    pre = jnp.concatenate([part_ref[j, :, width:].astype(F32) for j in range(parts)], axis=0)
    act = silu(pre)
    columns = unit_rows(act).T
    retain = jnp.broadcast_to(upright(retain_ref[pl.ds(place, 1), :]), (parts * tiles, HEAD_DIM))
    strength = jnp.broadcast_to(
        upright(strength_ref[pl.ds(place, 1), :]), (parts * tiles, HEAD_DIM)
    )
    slots = part_ref.shape[1]
    copies = []
    for j in range(parts):
        for t in range(tiles):
            h = j * tiles + t
            base = j * slots + t
            key = columns[:, base : base + 1]
            value = act[base + tiles : base + tiles + 1, :]
            old = s_ref[h]
            keep = retain[h : h + 1, :]
            recalled = jnp.sum(old * key, axis=0, keepdims=True)
            correction = (value - keep * recalled) * strength[h : h + 1, :]
            new[h] = keep * old + key * correction
        copies.append(
            pltpu.make_async_copy(
                new.at[pl.ds(j * tiles, tiles)], new_hbm.at[pl.ds(j * tiles, tiles)], sems.at[j]
            )
        )
        copies[-1].start()
    up = jnp.dot(normed, wu_ref[...], preferred_element_type=F32) * scale
    hidden = (silu(gate) * up).astype(BF16)
    for s in range(parts):
        hid_ref[s] = hidden
    for copy in copies:
        copy.wait()


def down_kernel(place_ref, hid_ref, res_ref, w_ref, out_ref, *, parts):
    units = hid_ref.shape[2]
    total = res_ref[place_ref[0]].astype(F32)
    for s in range(parts):
        total = total + jnp.dot(
            hid_ref[s], w_ref[s * units : (s + 1) * units, :], preferred_element_type=F32
        )
    out_ref[...] = total.astype(BF16)


def fast_body(
    tokens, old_state, mixer_gain, w_query, w_key, w_value, w_outgate, w_decay, w_write,
    decay_log, decay_bias, head_gain, w_output, channel_gain, w_gate, w_up, w_down, *, parts,
):
    rows, share = tokens.shape
    width = share * parts
    heads = old_state.shape[1]
    tiles = share // HEAD_DIM
    units = w_gate.shape[1]
    shape = jax.ShapeDtypeStruct
    place = lax.axis_index("kv").astype(jnp.int32).reshape(1)
    smem = pl.BlockSpec(memory_space=pltpu.SMEM)
    vmem = pl.BlockSpec(memory_space=pltpu.VMEM)
    hbm = pl.BlockSpec(memory_space=pltpu.HBM)
    states = (heads, HEAD_DIM, HEAD_DIM)
    state = old_state[0]

    which = lax.axis_index("tp").astype(jnp.int32).reshape(1)
    tokens, place, which = lax.optimization_barrier((tokens, place, which))
    slab = shape((tiles * (HEAD_DIM + rows), HEAD_DIM), BF16)
    sent = call(
        functools.partial(pack_kernel, parts=parts, tiles=tiles),
        [slab] * parts,
        (place, which, pltpu.with_memory_space_constraint(tokens, pltpu.HBM),
         pltpu.with_memory_space_constraint(state, pltpu.HBM)),
        scratch=[
            pltpu.VMEM((parts, tiles) + states[1:], F32),
            pltpu.VMEM((rows, share), BF16),
            pltpu.SemaphoreType.DMA((parts + 1,)),
        ],
        spaces=[smem, smem, hbm, hbm],
        span=1,
    )
    slabs = swap(sent)
    turned = shape((width, units), BF16)
    wide_gate, wide_up = call(
        turn_kernel,
        (turned, turned),
        (sent[0], pltpu.with_memory_space_constraint(w_gate.T, pltpu.HBM),
         pltpu.with_memory_space_constraint(w_up.T, pltpu.HBM)),
        scratch=[
            pltpu.VMEM((2, units, width), BF16),
            pltpu.SemaphoreType.DMA((2 * pl.cdiv(units, HEAD_DIM),)),
        ],
        spaces=[vmem, hbm, hbm],
        limit=16,
        span=40,
    )
    slabs, wide_gate, wide_up = lax.optimization_barrier((slabs, wide_gate, wide_up))
    part, wide, retain, strength = call(
        functools.partial(heads_kernel, parts=parts, tiles=tiles),
        (
            shape((parts, rows, width + HEAD_DIM), BF16),
            shape((rows, width), BF16),
            shape((rows, heads), F32),
            shape((rows, heads), F32),
        ),
        (
            place, which, mixer_gain.reshape(1, width), w_query, w_key, w_value, w_outgate,
            w_decay.T, w_write.T, decay_log.reshape(1, heads), decay_bias.reshape(1, heads),
            head_gain.reshape(1, HEAD_DIM), w_output, *slabs,
        ),
        scratch=[
            pltpu.VMEM((rows, rows, HEAD_DIM), F32),
            pltpu.VMEM((parts, tiles * rows, HEAD_DIM), F32),
        ],
        spaces=[smem] * 2 + [vmem] * (11 + parts),
    )
    part = exchange(part)
    hidden, residual, new_state = call(
        functools.partial(mixer_kernel, parts=parts, tiles=tiles),
        (
            shape((parts, rows, units), BF16),
            shape((parts, rows, share), BF16),
            shape(states, F32),
        ),
        (
            place, part, wide, channel_gain.reshape(1, width), retain, strength, state,
            wide_gate, wide_up,
        ),
        scratch=[pltpu.VMEM(states, F32), pltpu.SemaphoreType.DMA((parts,))],
        spaces=[smem] + [vmem] * 8,
        outs=[vmem, vmem, hbm],
    )
    hidden = exchange(hidden)
    mixed = call(
        functools.partial(down_kernel, parts=parts),
        shape((rows, share), BF16),
        (place, hidden, residual, w_down),
        spaces=[smem] + [vmem] * 3,
    )
    return mixed, new_state[None]


def body(
    tokens, old_state, mixer_gain, w_query, w_key, w_value, w_outgate, w_decay, w_write,
    decay_log, decay_bias, head_gain, w_output, channel_gain, w_gate, w_up, w_down, *, parts,
):
    rows, share = tokens.shape
    width = share * parts
    local_rows, heads = old_state.shape[:2]
    head_cols = w_query.shape[1]
    place = lax.axis_index("kv")

    tok_wide = gather_kv(tokens, parts).transpose(1, 0, 2).reshape(rows, width).astype(F32)
    scale_in = norm_scale(tok_wide)
    normed = (tok_wide * mixer_gain).astype(BF16)

    def project(weight):
        return (jnp.dot(normed, weight, preferred_element_type=F32) * scale_in).astype(BF16)

    packed = jnp.stack([project(w) for w in (w_query, w_key, w_value, w_outgate)], axis=1)
    packed = exchange(packed.reshape(parts, local_rows, 4, head_cols))

    own_normed = lax.dynamic_slice_in_dim(normed, place * local_rows, local_rows, 0)
    own_scale = lax.dynamic_slice_in_dim(scale_in, place * local_rows, local_rows, 0)
    decay_pre = jnp.dot(own_normed, w_decay, preferred_element_type=F32) * own_scale
    write_pre = jnp.dot(own_normed, w_write, preferred_element_type=F32) * own_scale

    def by_head(index):
        chosen = packed[:, :, index].transpose(1, 0, 2)
        return chosen.reshape(local_rows, heads, HEAD_DIM).astype(F32)

    queries = unit_rows(jax.nn.silu(by_head(0))) * HEAD_DIM ** (-0.5)
    keys_unit = unit_rows(jax.nn.silu(by_head(1)))
    values_act = jax.nn.silu(by_head(2))
    strength = jax.nn.sigmoid(write_pre)
    retain = jnp.exp(-jnp.exp(decay_log) * jax.nn.softplus(decay_pre + decay_bias))
    recalled = jnp.einsum("bhkv,bhk->bhv", old_state, keys_unit, precision=lax.Precision.HIGHEST)
    correction = values_act - retain[..., None] * recalled
    new_state = (
        retain[..., None, None] * old_state
        + (strength[..., None] * keys_unit)[..., :, None] * correction[..., None, :]
    )
    readout = jnp.einsum("bhkv,bhk->bhv", new_state, queries, precision=lax.Precision.HIGHEST)
    gated_read = readout * norm_scale(readout) * head_gain * jax.nn.silu(by_head(3))
    gated_read = gated_read.reshape(local_rows, parts, head_cols).astype(BF16)
    read_cols = exchange(gated_read.transpose(1, 0, 2)).reshape(rows, head_cols)

    partial_out = jnp.dot(read_cols, w_output, preferred_element_type=F32)
    mixer_out = exchange(partial_out.reshape(rows, parts, share).transpose(1, 0, 2)).sum(0)
    own_residual = (tokens.astype(F32) + mixer_out).astype(BF16)
    residual = gather_kv(own_residual, parts).transpose(1, 0, 2).reshape(rows, width)
    residual_wide = residual.astype(F32)
    scale_mid = norm_scale(residual_wide)
    normed_mid = (residual_wide * channel_gain).astype(BF16)
    gate_act = jnp.dot(normed_mid, w_gate, preferred_element_type=F32) * scale_mid
    upward = jnp.dot(normed_mid, w_up, preferred_element_type=F32) * scale_mid
    hidden = (jax.nn.silu(gate_act) * upward).astype(BF16)
    hidden = gather_kv(hidden, parts).transpose(1, 0, 2).reshape(rows, -1)
    down_sum = jnp.dot(hidden, w_down, preferred_element_type=F32)
    mixed = (own_residual.astype(F32) + down_sum).astype(BF16)
    return (mixed, new_state)


def solution(mesh):
    parts = mesh.shape["kv"]
    rows, states = P(("tp", "dp"), "kv"), P(("tp", "dp", "kv"), None, None, None)
    cols = P(None, "kv")
    in_specs = (rows, states, P(), cols, cols, cols, cols, P(), P(), P(), P(), P())
    in_specs += (P("kv", None), P(), cols, cols, cols)

    def step(*args):
        tokens, old_state = args[:2]
        share = tokens.shape[1]
        fits = (
            share % HEAD_DIM == 0
            and 2 * (share // HEAD_DIM) <= tokens.shape[0]
            and old_state.shape[0] == 1
            and tokens.shape[0] == parts == 8
            and args[3].shape[1] == share
            and args[14].shape[1] % 16 == 0
        )
        return (fast_body if fits else body)(*args, parts=parts)

    return jax.shard_map(
        step, mesh=mesh, in_specs=in_specs, out_specs=(rows, states), check_vma=False
    )
```
